256 devices in a mesh: sp: 64 (over z, x, core), tp: 4 (over y).
Axes of the slice: x: 4, y: 4, z: 8, core: 2. Of those that a mesh axis runs over, the one named last changes fastest.
Arguments:
- resid: bfloat16 [16384, 2048], P(('sp', 'tp')), may hold values from -6 to 6
- query_wide: bfloat16 [16384, 768], P('sp', 'tp'), may hold values from -2000 to 2000
- query_narrow: bfloat16 [16384, 512], P('sp', 'tp'), may hold values from -2000 to 2000
- latent: bfloat16 [16384, 256], P('sp'), may hold values from -6 to 6
- rope_key: bfloat16 [16384, 64], P('sp'), may hold values from -6 to 6
- latent_gain: float32 [256], replicated, may hold values from 0.1 to 1.9
- key_up_wide: bfloat16 [256, 512], replicated, may hold values from -0.375 to 0.375
- value_up_wide: bfloat16 [256, 512], replicated, may hold values from -0.375 to 0.375
- key_up_narrow: bfloat16 [256, 256], replicated, may hold values from -0.375 to 0.375
- value_up_narrow: bfloat16 [256, 256], replicated, may hold values from -0.375 to 0.375
- out_wide: bfloat16 [512, 2048], P('tp'), may hold values from -0.21875 to 0.21875
- out_narrow: bfloat16 [256, 2048], P('tp'), may hold values from -0.21875 to 0.21875
- attn_gain: float32 [2048], replicated, may hold values from 0.1 to 1.9
- ffn_gain: float32 [2048], replicated, may hold values from 0.1 to 1.9
- moe_gain: float32 [2048], replicated, may hold values from 0.1 to 1.9
- routes: int32 [16384, 2], P(('sp', 'tp')), may hold values from 0 to 63, all different within a row; in each aligned block of 64 rows (0 to 63, 64 to 127, ...) at most 3 rows name the same one
- route_logit: float32 [16384, 2], P(('sp', 'tp')), may hold values from -8 to 8
- expert_gate: bfloat16 [64, 2048, 3584], P('sp', None, 'tp'), may hold values from -0.125 to 0.125
- expert_up: bfloat16 [64, 2048, 3584], P('sp', None, 'tp'), may hold values from -0.125 to 0.125
- expert_down: bfloat16 [64, 3584, 2048], P('sp', 'tp'), may hold values from -0.09375 to 0.09375
Outputs:
- mixed: bfloat16 [16384, 2048], P(('sp', 'tp'))
The draws below stay inside these ranges and needn't reach their ends.
Inputs may be any that keep to these rules, and one draw needn't show every extreme that they name: `routes`: in each aligned block of 64 rows no expert is named by more than 3 rows, and a row's experts differ.
All inputs are finite; a program needn't handle non-finite values.
Results may differ from the reference program's by a relative error of at most 0.033.
Values may be sent and summed in bfloat16 or wider, within the bound.
A program may use at most 128 MiB of HBM per device.

```python
import math
import jax
import jax.numpy as jnp
import numpy as np
from jax import lax

D = 2048
HW = 4
HN = 4
NOPE_W = 128
V_W = 128
NOPE_N = 64
V_N = 64
ROPE = 64
KVR = 256
EFF = 3584
TOP = 2
SEQ = 16384
ROWS = 64
EXPERTS = 64
CAP = 3
N_TP = 4


def spiked(key, row_count, col_count):
    base = jnp.clip(jax.random.normal(key, (row_count, col_count), jnp.float32), -6.0, 6.0)
    return base.astype(jnp.bfloat16)


def draw_query_wide(key, part):
    return spiked(jax.random.fold_in(key, 11), SEQ, HW * (NOPE_W + ROPE))


def draw_query_narrow(key, part):
    return spiked(jax.random.fold_in(key, 13), SEQ, HN * (NOPE_N + ROPE))


def block_scale(stream_key, dims, split, smallest, top_value):
    level = 1.0
    for axis_at, blocks in split:
        steps = jax.random.uniform(jax.random.fold_in(jax.random.fold_in(stream_key, 6), axis_at), (blocks,), jnp.float32, smallest / len(split), top_value / len(split))
        level = level * jnp.repeat(jnp.exp(steps), dims[axis_at] // blocks).reshape((-1,) + (1,) * (len(dims) - 1 - axis_at))
    return level


def deal_out(stream_key, own, number, rows, number_of, top, bound, skew):
    order = jax.random.permutation(stream_key, number_of)
    packed, ordinary = portions_of(number_of, rows * top, bound, skew, True), portions_of(number_of, rows * top, bound, skew, False)
    places = jnp.arange(number_of)

    def named(tallies, offset_by):
        used = int((tallies > 0).sum())
        fixed = max(1, used // 4)
        moved = fixed + (places - fixed + offset_by * (used - fixed)) % max(1, number_of - fixed)
        return jnp.zeros((number_of,), jnp.int32).at[order[jnp.where(places < fixed, places, moved)]].set(jnp.asarray(tallies, jnp.int32))

    tallies = jnp.where(number % 4 == 0, named(packed, number // 4), named(ordinary, number - number // 4 - 1))
    mixed = jax.random.permutation(jax.random.fold_in(own, 3), number_of)
    giver, taker = mixed[0:number_of // 2 * 2:2], mixed[1:number_of // 2 * 2:2]
    room = jnp.minimum(tallies[giver] - 1, bound - tallies[taker]) // 2
    room = jnp.where((giver == order[0]) | (taker == order[0]) | (tallies[taker] == 0), 0, jnp.maximum(room, 0))
    moved = jax.random.randint(jax.random.fold_in(own, 4), (number_of // 2,), 0, 1 << 20) % (room + 1)
    tallies = tallies.at[giver].add(-moved).at[taker].add(moved)
    items = jnp.searchsorted(jnp.cumsum(tallies), jnp.arange(rows * top), side="right").astype(jnp.int32)
    listing = items.reshape(top, rows).T
    listing = listing[jax.random.permutation(jax.random.fold_in(own, 1), rows)]
    offset_by = jax.random.randint(jax.random.fold_in(own, 2), (rows, 1), 0, top)
    return jnp.take_along_axis(listing, (jnp.arange(top)[None, :] + offset_by) % top, axis=1)


def portions_of(count, total, most, skew, full):
    portions = [(1 << 20) // math.isqrt(grade ** skew) + 1 for grade in range(1, count + 1)]
    largest = most if full else min(most, max(-(-total // count), total * portions[0] // sum(portions)))
    least = 1 if total - largest >= count - 1 else 0
    counts, surplus = [largest] + [least] * (count - 1), total - largest - least * (count - 1)
    while surplus > 0:
        free = [i for i in range(1, count) if counts[i] < largest] or [i for i in range(1, count) if counts[i] < most]
        whole, left = sum([portions[i] for i in free]), surplus
        for i in free:
            extra = min(most - counts[i], max(1, left * portions[i] // whole), surplus)
            counts[i] = counts[i] + extra
            surplus = surplus - extra
    return np.array(counts)


def normal_values(key, extent, scale, most, pieces=(), kind=jnp.bfloat16):
    array = jax.random.normal(key, extent, jnp.float32) * scale
    if len(pieces) > 0:
        array = block_scale(key, extent, pieces, -0.22, 0.18) * array
    return jnp.clip(array, min=-most, max=most).astype(kind)


def setup_inputs(seed: int = 0) -> dict:
    seeds = jax.random.split(jax.random.key(seed), 21)
    resid = normal_values(seeds[0], (SEQ, D), 1.0, 6.0, ((0, 256),))
    query_wide = draw_query_wide(jax.random.fold_in(seeds[20], 71), 0)
    query_narrow = draw_query_narrow(jax.random.fold_in(seeds[20], 71), 0)
    latent = normal_values(seeds[3], (SEQ, KVR), 1.0, 6.0, ((0, 64),))
    rope_key = normal_values(seeds[4], (SEQ, ROPE), 1.0, 6.0, ((0, 64),))
    latent_gain = jnp.clip(1.0 + 0.18 * jax.random.normal(seeds[5], (KVR,), jnp.float32), 0.1, 1.9)
    key_up_wide = normal_values(seeds[6], (KVR, HW * NOPE_W), KVR ** -0.5, 0.375)
    value_up_wide = normal_values(seeds[7], (KVR, HW * V_W), KVR ** -0.5, 0.375)
    key_up_narrow = normal_values(seeds[8], (KVR, HN * NOPE_N), KVR ** -0.5, 0.375)
    value_up_narrow = normal_values(seeds[9], (KVR, HN * V_N), KVR ** -0.5, 0.375)
    out_wide = normal_values(seeds[10], (HW * V_W, D), (HW * V_W + HN * V_N) ** -0.5, 0.21875, ((0, 4),))
    out_narrow = normal_values(seeds[11], (HN * V_N, D), (HW * V_W + HN * V_N) ** -0.5, 0.21875, ((0, 4),))
    attn_gain = jnp.clip(1.0 + 0.18 * jax.random.normal(seeds[12], (D,), jnp.float32), 0.1, 1.9)
    ffn_gain = jnp.clip(1.0 + 0.18 * jax.random.normal(seeds[13], (D,), jnp.float32), 0.1, 1.9)
    moe_gain = jnp.clip(1.0 + 0.18 * jax.random.normal(seeds[14], (D,), jnp.float32), 0.1, 1.9)
    routes_keys = jax.random.split(jax.random.fold_in(seeds[15], 1), SEQ // ROWS)
    routes_turns = jax.random.permutation(jax.random.fold_in(seeds[15], 3), SEQ // ROWS)
    routes = jax.vmap(lambda own, number: deal_out(jax.random.fold_in(seeds[15], 2), own, number, ROWS, EXPERTS, TOP, CAP, 2))(routes_keys, routes_turns).reshape((SEQ, TOP))
    route_logit = normal_values(seeds[16], (SEQ, TOP), 1.5, 8.0, ((0, 256),), jnp.float32)
    expert_gate = normal_values(seeds[17], (EXPERTS, D, EFF), D ** -0.5, 0.125, ((0, 64), (2, 4)))
    expert_up = normal_values(seeds[18], (EXPERTS, D, EFF), D ** -0.5, 0.125, ((0, 64), (2, 4)))
    expert_down = normal_values(seeds[19], (EXPERTS, EFF, D), EFF ** -0.5, 0.09375, ((0, 64), (1, 4)))
    return {"resid": resid, "query_wide": query_wide, "query_narrow": query_narrow, "latent": latent, "rope_key": rope_key, "latent_gain": latent_gain, "key_up_wide": key_up_wide, "value_up_wide": value_up_wide, "key_up_narrow": key_up_narrow, "value_up_narrow": value_up_narrow, "out_wide": out_wide, "out_narrow": out_narrow, "attn_gain": attn_gain, "ffn_gain": ffn_gain, "moe_gain": moe_gain, "routes": routes, "route_logit": route_logit, "expert_gate": expert_gate, "expert_up": expert_up, "expert_down": expert_down}


EPS = 1e-06
THETA = 10000.0

def rms_scale(values, gain):
    return values * lax.rsqrt(lax.optimization_barrier(jnp.mean(values * values, axis=-1, keepdims=True)) + EPS) * gain.astype(jnp.float32)

def rotate(values, positions):
    half = values.shape[-1] // 2
    freq = THETA ** (-jnp.arange(half, dtype=jnp.float32) * 2.0 / values.shape[-1])
    angle = positions.astype(jnp.float32)[..., None] * freq
    cosine = jnp.cos(angle)
    sine = jnp.sin(angle)
    real = values.astype(jnp.float32)
    first = real[..., :half]
    second = real[..., half:]
    return jnp.concatenate([first * cosine - second * sine, second * cosine + first * sine], axis=-1).astype(jnp.bfloat16)

def contract(left, right):
    return lax.dot_general(left, right, (((1,), (1,)), ((), ())), preferred_element_type=jnp.float32)

def head_attend(q_nope, q_rope, k_nope, k_rope, values, factor):
    length = q_nope.shape[0]
    block = math.gcd(length, 512)

    def one_block(index):
        query_a = lax.dynamic_slice_in_dim(q_nope, index * block, block, 0)
        query_b = lax.dynamic_slice_in_dim(q_rope, index * block, block, 0)
        scores = (contract(query_a, k_nope) + contract(query_b, k_rope)) * factor
        top_score = lax.optimization_barrier(jnp.max(scores, axis=1, keepdims=True))
        weights = jnp.exp(scores - top_score)
        weight_sum = lax.optimization_barrier(jnp.sum(weights, axis=1, keepdims=True))
        summed = jnp.dot(weights.astype(jnp.bfloat16), values, preferred_element_type=jnp.float32)
        return (summed / weight_sum).astype(jnp.bfloat16)
    blocks = jnp.arange(length // block, dtype=jnp.int32)
    result = lax.map(one_block, blocks)
    return result.reshape(length, values.shape[1])

def rounded(values):
    return lax.optimization_barrier(values.astype(jnp.bfloat16)).astype(jnp.float32)

def reference(resid, query_wide, query_narrow, latent, rope_key, latent_gain, key_up_wide, value_up_wide, key_up_narrow, value_up_narrow, out_wide, out_narrow, attn_gain, ffn_gain, moe_gain, routes, route_logit, expert_gate, expert_up, expert_down):
    positions = jnp.arange(SEQ, dtype=jnp.int32)
    normed = rms_scale(latent.astype(jnp.float32), latent_gain).astype(jnp.bfloat16)
    turned_key = rotate(rope_key, positions)

    def expand(weight):
        return jnp.dot(normed, weight, preferred_element_type=jnp.float32).astype(jnp.bfloat16)
    keys_wide = expand(key_up_wide)
    vals_wide = expand(value_up_wide)
    keys_narrow = expand(key_up_narrow)
    vals_narrow = expand(value_up_narrow)
    q_wide = query_wide.reshape(SEQ, HW, NOPE_W + ROPE)
    q_narrow = query_narrow.reshape(SEQ, HN, NOPE_N + ROPE)
    wide_turn = rotate(q_wide[:, :, NOPE_W:], positions[:, None])
    narrow_turn = rotate(q_narrow[:, :, NOPE_N:], positions[:, None])
    wide_outs = []
    for head in range(HW):
        wide_outs.append(head_attend(q_wide[:, head, :NOPE_W], wide_turn[:, head], keys_wide[:, head * NOPE_W:(head + 1) * NOPE_W], turned_key, vals_wide[:, head * V_W:(head + 1) * V_W], (NOPE_W + ROPE) ** (-0.5)))
    narrow_outs = []
    for head in range(HN):
        narrow_outs.append(head_attend(q_narrow[:, head, :NOPE_N], narrow_turn[:, head], keys_narrow[:, head * NOPE_N:(head + 1) * NOPE_N], turned_key, vals_narrow[:, head * V_N:(head + 1) * V_N], (NOPE_N + ROPE) ** (-0.5)))
    o_wide = jnp.concatenate(wide_outs, axis=1)
    o_narrow = jnp.concatenate(narrow_outs, axis=1)
    wide_cols = HW // N_TP * V_W
    narrow_cols = HN // N_TP * V_N
    proj = jnp.zeros((SEQ, D), jnp.float32)
    for group in range(N_TP):
        part = jnp.dot(o_wide[:, group * wide_cols:(group + 1) * wide_cols], out_wide[group * wide_cols:(group + 1) * wide_cols], preferred_element_type=jnp.float32)
        part = part + jnp.dot(o_narrow[:, group * narrow_cols:(group + 1) * narrow_cols], out_narrow[group * narrow_cols:(group + 1) * narrow_cols], preferred_element_type=jnp.float32)
        proj = proj + rounded(part)
    stream = (resid.astype(jnp.float32) + rms_scale(proj, attn_gain)).astype(jnp.bfloat16)
    moe_in = rms_scale(stream.astype(jnp.float32), ffn_gain).astype(jnp.bfloat16)
    n_blocks = SEQ // ROWS
    pairs = ROWS * TOP
    chosen = routes.reshape(n_blocks, pairs)
    onehot = (chosen[:, :, None] == jnp.arange(EXPERTS, dtype=jnp.int32)[None, None, :]).astype(jnp.int32)
    before = jnp.cumsum(onehot, axis=1) - onehot
    slot = lax.optimization_barrier(jnp.sum(before * onehot, axis=2))
    dest = (chosen * CAP + slot).astype(jnp.int32)
    row_index = (jnp.arange(n_blocks, dtype=jnp.int32)[:, None] * ROWS + jnp.arange(pairs, dtype=jnp.int32)[None, :] // TOP).astype(jnp.int32)
    table = jnp.full((n_blocks, EXPERTS * CAP), -1, jnp.int32)
    table = table.at[jnp.arange(n_blocks, dtype=jnp.int32)[:, None], dest].set(row_index)
    per_expert = jnp.transpose(table.reshape(n_blocks, EXPERTS, CAP), (1, 0, 2)).reshape(EXPERTS, n_blocks * CAP)
    width = EFF // N_TP

    def one_expert(operands):
        index, w_gate, w_up, w_down = operands
        picked = moe_in[jnp.maximum(index, 0)]
        picked = jnp.where((index >= 0)[:, None], picked, jnp.zeros_like(picked))
        summed = jnp.zeros((index.shape[0], D), jnp.float32)
        for group in range(N_TP):
            gate = jnp.dot(picked, w_gate[:, group * width:(group + 1) * width], preferred_element_type=jnp.float32)
            upper = jnp.dot(picked, w_up[:, group * width:(group + 1) * width], preferred_element_type=jnp.float32)
            hidden = (jax.nn.silu(gate) * upper).astype(jnp.bfloat16)
            part = jnp.dot(hidden, w_down[group * width:(group + 1) * width], preferred_element_type=jnp.float32)
            summed = summed + rounded(part)
        return summed.astype(jnp.bfloat16)
    expert_out = lax.map(one_expert, (per_expert, expert_gate, expert_up, expert_down))
    by_block = jnp.transpose(expert_out.reshape(EXPERTS, n_blocks, CAP, D), (1, 0, 2, 3)).reshape(n_blocks, EXPERTS * CAP, D)
    gathered = by_block[jnp.arange(n_blocks, dtype=jnp.int32)[:, None], dest].reshape(SEQ, TOP, D)
    share = jax.nn.softmax(route_logit.astype(jnp.float32), axis=-1)
    branch = lax.optimization_barrier(jnp.sum(share[:, :, None] * gathered.astype(jnp.float32), axis=1))
    return (stream.astype(jnp.float32) + rms_scale(branch, moe_gain)).astype(jnp.bfloat16)
```

```python
import functools
import math

import jax
import jax.numpy as jnp
from jax import lax
from jax.experimental import pallas as pl
from jax.experimental.pallas import tpu as pltpu
from jax.sharding import Mesh
from jax.sharding import PartitionSpec as P

NOPE_W = 128
V_W = 128
NOPE_N = 64
V_N = 64
ROPE = 64
SP = ("sp_0", "sp_1", "sp_2")
SP_TP = ("sp_0", "sp_1", "sp_2", "tp")
NZ, NX, NC, NT = 8, 4, 2, 4
TOK = 256
SUB = 64
LOG2E = math.log2(math.e)
MESH_ID = pl.DeviceIdType.MESH

EPS = 1e-06
THETA = 10000.0


def send(src, dst, send_sem, recv_sem, where):
    copy = pltpu.make_async_remote_copy(
        src_ref=src,
        dst_ref=dst,
        send_sem=send_sem,
        recv_sem=recv_sem,
        device_id=where,
        device_id_type=MESH_ID,
    )
    copy.start()
    return copy


def greet(peers):
    barrier = pltpu.get_barrier_semaphore()
    for peer in peers:
        pl.semaphore_signal(barrier, inc=1, device_id=peer, device_id_type=MESH_ID)
    pl.semaphore_wait(barrier, len(peers))


def mm(a, b):
    return jnp.dot(a, b, preferred_element_type=jnp.float32)


def mm_nt(a, b):
    return lax.dot_general(a, b, (((1,), (1,)), ((), ())), preferred_element_type=jnp.float32)


FACTOR_W = (NOPE_W + ROPE) ** (-0.5) * LOG2E
FACTOR_N = (NOPE_N + ROPE) ** (-0.5) * LOG2E


def attention_kernel(
    q_in,
    kv_in,
    w_in,
    out_ref,
    qbuf,
    kvbuf,
    kw_s,
    kn_s,
    vw_s,
    vn_s,
    top_w,
    top_n,
    acc_w,
    acc_n,
    osend,
    orecv,
    ysend,
    yrecv,
    q_ss,
    q_rs,
    f_ss,
    f_rs,
    b_ss,
    b_rs,
    d_ss,
    d_rs,
    o_ss,
    o_rs,
    y_ss,
    y_rs,
):
    z = lax.axis_index("sp_0")
    x = lax.axis_index("sp_1")
    core = lax.axis_index("sp_2")
    y = lax.axis_index("tp")
    up = {"sp_0": lax.rem(z + 1, NZ)}
    down = {"sp_0": lax.rem(z + NZ - 1, NZ)}
    sibling = {"sp_2": 1 - core}
    xs = {j: {"sp_1": lax.rem(x + j, NX)} for j in range(1, NX)}
    ys = {j: {"tp": lax.rem(y + j, NT)} for j in range(1, NT)}
    greet([up, down, sibling] + list(xs.values()) + list(ys.values()))

    half = TOK // 2

    def piece(r):
        return kv_in if r == 0 else kvbuf.at[r, 0]

    waits = []
    fwd = {1: send(kv_in, kvbuf.at[1, 0], f_ss.at[1], f_rs.at[1], up)}
    bwd = {1: send(kv_in, kvbuf.at[7, 0], b_ss.at[1], b_rs.at[1], down)}
    across = {0: send(kv_in, kvbuf.at[0, 1], d_ss.at[0], d_rs.at[0], sibling)}
    qcopies = {}
    for j in (1, 3, 2):
        qcopies[j] = send(q_in, qbuf.at[j], q_ss.at[j], q_rs.at[j], xs[j])

    lane = lax.broadcasted_iota(jnp.int32, (2 * TOK, 128), 1)
    vw_s[:, 128:] = jnp.ones((2 * TOK, 128), jnp.bfloat16)

    def expand(r):
        w = w_in[...]
        if r == 0:
            kv = jnp.concatenate([kv_in[...], kvbuf[0, 1]], axis=0)
        else:
            kv = kvbuf[r].reshape(2 * TOK, 384)
        full = mm(kv[:, :256], w)
        tail = kv[:, 256:]
        kw_s[:, :128] = full[:, :128].astype(jnp.bfloat16)
        kw_s[:, 128:] = tail
        kn_s[...] = jnp.where(
            lane < 64, full[:, 128:256], tail.astype(jnp.float32)
        ).astype(jnp.bfloat16)
        vw_s[:, :128] = full[:, 256:384].astype(jnp.bfloat16)
        vn_s[...] = jnp.where(lane < 64, full[:, 384:], 1.0).astype(jnp.bfloat16)

    def one_head(q, keys, values, top, acc, j, factor, first):
        scores = mm_nt(q, keys)
        best = jnp.max(scores, axis=1, keepdims=True)
        if not first:
            old = top[j]
            new = jnp.maximum(old, best)
            shrink = jnp.exp2((old - new) * factor)
            best = new[:, :1]
        else:
            new = jnp.broadcast_to(best, (TOK, 128))
        weights = jnp.exp2((scores - best) * factor).astype(jnp.bfloat16)
        summed = mm(weights, values)
        if not first:
            width = summed.shape[1]
            wide = shrink if width == 128 else jnp.concatenate([shrink, shrink], axis=1)
            summed = acc[j] * wide + summed
        acc[j] = summed
        top[j] = new

    def attend(j, q, first):
        one_head(q[:, :256], kw_s[...], vw_s[...], top_w, acc_w, j, FACTOR_W, first)
        one_head(q[:, 256:], kn_s[...], vn_s[...], top_n, acc_n, j, FACTOR_N, first)

    def all_queries(first):
        attend(0, q_in[...], first)

        def body(j, carry):
            attend(j, qbuf[j], first)
            return carry

        lax.fori_loop(1, NX, body, 0)

    across[0].wait_recv()
    expand(0)
    attend(0, q_in[...], True)
    for j in (1, 3, 2):
        qcopies[j].wait_recv()

    def first_body(j, carry):
        attend(j, qbuf[j], True)
        return carry

    lax.fori_loop(1, NX, first_body, 0)

    for k in range(1, 4):
        fwd[k].wait_recv()
        if k < 3:
            fwd[k + 1] = send(
                kvbuf.at[k, 0], kvbuf.at[k + 1, 0], f_ss.at[k + 1], f_rs.at[k + 1], up
            )
        else:
            fwd[4] = send(
                kvbuf.at[3, 0, pl.ds(0, half)],
                kvbuf.at[4, 0, pl.ds(0, half)],
                f_ss.at[4],
                f_rs.at[4],
                up,
            )
        across[k] = send(kvbuf.at[k, 0], kvbuf.at[k, 1], d_ss.at[k], d_rs.at[k], sibling)
        bwd[k].wait_recv()
        if k < 3:
            bwd[k + 1] = send(
                kvbuf.at[8 - k, 0], kvbuf.at[7 - k, 0], b_ss.at[k + 1], b_rs.at[k + 1], down
            )
        else:
            bwd[4] = send(
                kvbuf.at[5, 0, pl.ds(half, half)],
                kvbuf.at[4, 0, pl.ds(half, half)],
                b_ss.at[4],
                b_rs.at[4],
                down,
            )
        across[8 - k] = send(
            kvbuf.at[8 - k, 0], kvbuf.at[8 - k, 1], d_ss.at[8 - k], d_rs.at[8 - k], sibling
        )
        across[k].wait_recv()
        expand(k)
        all_queries(False)
        across[8 - k].wait_recv()
        expand(8 - k)
        all_queries(False)

    fwd[4].wait_recv()
    across[4] = send(
        kvbuf.at[4, 0, pl.ds(0, half)],
        kvbuf.at[4, 1, pl.ds(0, half)],
        d_ss.at[4],
        d_rs.at[4],
        sibling,
    )
    bwd[4].wait_recv()
    across[8] = send(
        kvbuf.at[4, 0, pl.ds(half, half)],
        kvbuf.at[4, 1, pl.ds(half, half)],
        d_ss.at[8],
        d_rs.at[8],
        sibling,
    )
    across[4].wait_recv()
    across[8].wait_recv()
    expand(4)

    lane_q = lax.broadcasted_iota(jnp.int32, (TOK, 128), 1)

    def three(value):
        high = value.astype(jnp.bfloat16).astype(jnp.float32)
        rest = value - high
        middle = rest.astype(jnp.bfloat16).astype(jnp.float32)
        return high, middle, rest - middle

    def finish(j, ref):
        total_w = acc_w[j, :, 128:]
        ref[:, :128] = (acc_w[j, :, :128] / total_w).astype(jnp.bfloat16)
        both = acc_n[j]
        total_n = pltpu.roll(both, 64, 1)
        tail = both / total_n
        level_w = top_w[j] * FACTOR_W + jnp.log2(total_w)
        level_n = top_n[j] * FACTOR_N + jnp.log2(both)
        at = 64
        for part in three(level_w) + three(level_n):
            tail = jnp.where(lane_q == at, part, tail)
            at += 1
        ref[:, 128:] = tail.astype(jnp.bfloat16)

    ocopies = {}
    for j in (2, 1, 3):
        attend(j, qbuf[j], False)
        finish(j, osend.at[j])
        ocopies[j] = send(
            osend.at[j], orecv.at[j], o_ss.at[j], o_rs.at[j], {"sp_1": lax.rem(x + NX - j, NX)}
        )
    attend(0, q_in[...], False)
    finish(0, osend.at[0])
    for j in (1, 3, 2):
        ocopies[j].wait_recv()

    tails = [osend[0, :, 128:].astype(jnp.float32)] + [
        orecv[j, :, 128:].astype(jnp.float32) for j in range(1, NX)
    ]
    mains = [osend[0, :, :128]] + [orecv[j, :, :128] for j in range(1, NX)]

    def shares(at):
        levels = [(t[:, at : at + 1] + t[:, at + 1 : at + 2]) + t[:, at + 2 : at + 3] for t in tails]
        best = functools.reduce(jnp.maximum, levels)
        parts = [jnp.exp2(level - best) for level in levels]
        total = functools.reduce(jnp.add, parts)
        return [part / total for part in parts]

    share_w = shares(64)
    share_n = shares(67)
    merged_w = functools.reduce(
        jnp.add, [m.astype(jnp.float32) * s for m, s in zip(mains, share_w)]
    )
    merged_n = functools.reduce(jnp.add, [t * s for t, s in zip(tails, share_n)])
    ysend[:, :128] = merged_w.astype(jnp.bfloat16)
    ysend[:, 128:] = jnp.where(lane_q < 64, merged_n, 0.0).astype(jnp.bfloat16)
    ycopies = {}
    for j in (2, 1, 3):
        rows = pl.ds(pl.multiple_of(lax.rem(y + j, NT) * SUB, SUB), SUB)
        ycopies[j] = send(ysend.at[rows], yrecv.at[j], y_ss.at[j], y_rs.at[j], ys[j])
    out_ref[0] = ysend[pl.ds(pl.multiple_of(y * SUB, SUB), SUB)]
    for j in range(1, NT):
        ycopies[j].wait_recv()
        out_ref[j] = yrecv[j]
    for group in (fwd, bwd, across, qcopies, ocopies, ycopies):
        for copy in group.values():
            copy.wait_send()


def attention(q, kv, weights):
    bf = jnp.bfloat16
    f32 = jnp.float32
    dma = pltpu.SemaphoreType.DMA
    return pl.pallas_call(
        attention_kernel,
        out_shape=jax.ShapeDtypeStruct((NT, SUB, 256), bf),
        in_specs=[pl.BlockSpec(memory_space=pltpu.VMEM)] * 3,
        out_specs=pl.BlockSpec(memory_space=pltpu.VMEM),
        scratch_shapes=[
            pltpu.VMEM((NX, TOK, 384), bf),
            pltpu.VMEM((NZ, NC, TOK, 384), bf),
            pltpu.VMEM((2 * TOK, 256), bf),
            pltpu.VMEM((2 * TOK, 128), bf),
            pltpu.VMEM((2 * TOK, 256), bf),
            pltpu.VMEM((2 * TOK, 128), bf),
            pltpu.VMEM((NX, TOK, 128), f32),
            pltpu.VMEM((NX, TOK, 128), f32),
            pltpu.VMEM((NX, TOK, 256), f32),
            pltpu.VMEM((NX, TOK, 128), f32),
            pltpu.VMEM((NX, TOK, 256), bf),
            pltpu.VMEM((NX, TOK, 256), bf),
            pltpu.VMEM((TOK, 256), bf),
            pltpu.VMEM((NT, SUB, 256), bf),
            dma((NX,)),
            dma((NX,)),
            dma((5,)),
            dma((5,)),
            dma((5,)),
            dma((5,)),
            dma((9,)),
            dma((9,)),
            dma((NX,)),
            dma((NX,)),
            dma((NT,)),
            dma((NT,)),
        ],
        compiler_params=pltpu.CompilerParams(
            collective_id=0, has_side_effects=True, vmem_limit_bytes=40 * 1024 * 1024
        ),
        cost_estimate=pl.CostEstimate(
            flops=12_000_000_000, bytes_accessed=4_000_000, transcendentals=8_400_000
        ),
        name="attention",
    )(q, kv, weights)


def in_blocks(array, dim, length):
    lengths = array.shape
    tiles = array.reshape(*lengths[:dim], length, lengths[dim] // length, *lengths[dim + 1 :])
    return jnp.moveaxis(tiles, dim, 0)


def sent_and_summed(array, axis, dim):
    length = lax.axis_size(axis)
    tiles = lax.all_to_all(in_blocks(array, dim, length), axis, 0, 0, tiled=True)
    return jnp.sum(tiles.astype(jnp.float32), axis=0)


def sent_to_all(array, axis):
    copies = jnp.broadcast_to(array, (lax.axis_size(axis), *array.shape))
    return lax.all_to_all(copies, axis, split_axis=0, concat_axis=0, tiled=True)


def in_order(tiles, dim):
    tiles = jnp.moveaxis(tiles, 0, dim)
    lengths = tiles.shape
    return tiles.reshape(*lengths[:dim], lengths[dim] * lengths[dim + 1], *lengths[dim + 2 :])


def collect(array, axis, dim):
    tiles = sent_to_all(array, axis)
    return in_order(tiles, dim)


def moved_by_axis(tiles, axes, order):
    inside = tiles.shape[1:]
    result = tiles.reshape(*(lax.axis_size(a) for a in axes), *inside)
    for k in order:
        result = lax.all_to_all(result, axes[k], k, k, tiled=True)
    return result.reshape(-1, *inside)


def core_and_chips(array, groups, order, split_dim, concat_dim):
    length = lax.axis_size(groups[0]) * lax.axis_size(groups[1])
    tiles = in_blocks(array, split_dim, length)
    return in_order(moved_by_axis(tiles, groups, order), concat_dim)


def rms_scale(values, gain):
    return values * lax.rsqrt(jnp.mean(values * values, axis=-1, keepdims=True) + EPS) * gain


def rotate(values, positions):
    half = values.shape[-1] // 2
    freq = THETA ** (-jnp.arange(half, dtype=jnp.float32) * 2.0 / values.shape[-1])
    angle = positions.astype(jnp.float32)[..., None] * freq
    cosine = jnp.cos(angle)
    sine = jnp.sin(angle)
    real = values.astype(jnp.float32)
    first = real[..., :half]
    second = real[..., half:]
    return jnp.concatenate(
        [first * cosine - second * sine, second * cosine + first * sine], axis=-1
    ).astype(jnp.bfloat16)


def local(
    resid,
    query_wide,
    query_narrow,
    latent,
    rope_key,
    latent_gain,
    key_up_wide,
    value_up_wide,
    key_up_narrow,
    value_up_narrow,
    out_wide,
    out_narrow,
    attn_gain,
    ffn_gain,
    moe_gain,
    routes,
    route_logit,
    expert_gate,
    expert_up,
    expert_down,
):
    tp_rank = lax.axis_index("tp")
    out_mine = jnp.concatenate([out_wide, out_narrow], axis=0)
    out_rows = [out_mine] + [
        lax.ppermute(out_mine, "tp", [(i, (i + j) % NT) for i in range(NT)]) for j in range(1, NT)
    ]
    positions = lax.axis_index(SP) * TOK + jnp.arange(TOK, dtype=jnp.int32)
    normed = rms_scale(latent.astype(jnp.float32), latent_gain).astype(jnp.bfloat16)
    turns = rotate(
        jnp.stack([rope_key, query_wide[:, NOPE_W:], query_narrow[:, NOPE_N:]]), positions
    )
    kv = jnp.concatenate([normed, turns[0], turns[0]], axis=1)
    zeros = jnp.zeros((TOK, 64), jnp.bfloat16)
    q = jnp.concatenate(
        [query_wide[:, :NOPE_W], turns[1], zeros, query_narrow[:, :NOPE_N], turns[2]], axis=1
    )

    def my_columns(weight, count):
        mine = lax.dynamic_slice_in_dim(weight, tp_rank * count, count, 1)
        return mine if count == 128 else jnp.concatenate([mine, jnp.zeros_like(mine)], axis=1)

    weights = jnp.concatenate(
        [
            my_columns(key_up_wide, NOPE_W),
            my_columns(key_up_narrow, NOPE_N),
            my_columns(value_up_wide, V_W),
            my_columns(value_up_narrow, V_N),
        ],
        axis=1,
    )
    heads = attention(q, kv, weights)
    proj = jnp.zeros((SUB, 2048), jnp.float32)
    for j in range(NT):
        part = jnp.dot(
            heads[j, :, : V_W + V_N], out_rows[j], preferred_element_type=jnp.float32
        )
        proj = proj + part.astype(jnp.bfloat16).astype(jnp.float32)
    stream = (resid.astype(jnp.float32) + rms_scale(proj, attn_gain)).astype(jnp.bfloat16)
    moe_in = rms_scale(stream.astype(jnp.float32), ffn_gain).astype(jnp.bfloat16)
    row_count = resid.shape[0]
    top_count = routes.shape[1]
    experts = lax.axis_size(SP)
    capacity = (3 * row_count * top_count + 2 * experts - 1) // (2 * experts)
    chosen = routes.reshape(-1)
    onehot = (chosen[:, None] == jnp.arange(experts, dtype=jnp.int32)[None, :]).astype(jnp.int32)
    before = jnp.cumsum(onehot, axis=0) - onehot
    slot = jnp.sum(before * onehot, axis=1)
    dest = (chosen * capacity + slot).reshape(row_count, top_count)
    slot_ids = jnp.arange(experts * capacity, dtype=jnp.int32)
    placing = jnp.any(slot_ids[:, None, None] == dest[None, :, :], axis=2).astype(jnp.bfloat16)
    outgoing = jnp.dot(placing, moe_in, preferred_element_type=jnp.float32).astype(jnp.bfloat16)
    outgoing = outgoing.reshape(experts, capacity, moe_in.shape[1])
    gathered = collect(
        lax.all_to_all(outgoing, SP, split_axis=0, concat_axis=0, tiled=True), "tp", 0
    )
    flat = gathered.reshape(-1, gathered.shape[2])
    gate = jnp.dot(flat, expert_gate[0], preferred_element_type=jnp.float32)
    upper = jnp.dot(flat, expert_up[0], preferred_element_type=jnp.float32)
    hidden = (jax.nn.silu(gate) * upper).astype(jnp.bfloat16)
    partial_out = jnp.dot(hidden, expert_down[0], preferred_element_type=jnp.float32).reshape(
        gathered.shape
    )
    summed = sent_and_summed(partial_out.astype(jnp.bfloat16), "tp", 0).astype(jnp.bfloat16)
    returned = core_and_chips(summed, (("sp_0", "sp_1"), "sp_2"), (0, 1), 0, 0)
    flat_back = returned.reshape(experts * capacity, returned.shape[2])
    picked = flat_back[dest]
    share = jax.nn.softmax(route_logit, axis=-1)
    branch = jnp.sum(share[:, :, None] * picked.astype(jnp.float32), axis=1)
    return (stream.astype(jnp.float32) + rms_scale(branch, moe_gain)).astype(jnp.bfloat16)


def solution(mesh):
    split = Mesh(mesh.devices.reshape(8, 4, 2, mesh.shape["tp"]), ("sp_0", "sp_1", "sp_2", "tp"))
    in_specs = (
        P(SP_TP, None),
        P(SP, "tp"),
        P(SP, "tp"),
        P(SP, None),
        P(SP, None),
        P(),
        P(),
        P(),
        P(),
        P(),
        P("tp", None),
        P("tp", None),
        P(),
        P(),
        P(),
        P(SP_TP, None),
        P(SP_TP, None),
        P(SP, None, "tp"),
        P(SP, None, "tp"),
        P(SP, "tp", None),
    )
    out_specs = P(SP_TP, None)
    return jax.shard_map(local, mesh=split, in_specs=in_specs, out_specs=out_specs, check_vma=False)
```

```python
import functools
import math

import jax
import jax.numpy as jnp
from jax import lax
from jax.experimental import pallas as pl
from jax.experimental.pallas import tpu as pltpu
from jax.sharding import Mesh
from jax.sharding import PartitionSpec as P

NOPE_W = 128
NOPE_N = 64
ROPE = 64
SP = ("sp_0", "sp_1", "sp_2")
SP_TP = ("sp_0", "sp_1", "sp_2", "tp")
NZ, NX, NC, NT = 8, 4, 2, 4
TOK = 256
SUB = 64
D = 2048
LOG2E = math.log2(math.e)
MESH_ID = pl.DeviceIdType.MESH

EPS = 1e-06
THETA = 10000.0

GROUP = NX * NC
SLOTS = 3
PARTS = 2
LANES = D // PARTS
CHUNKS = SLOTS * PARTS
ROWS = NZ * GROUP
HID = 896
HALF = ROWS // 2

FACTOR_W = (NOPE_W + ROPE) ** (-0.5) * LOG2E
FACTOR_N = (NOPE_N + ROPE) ** (-0.5) * LOG2E

BF = jnp.bfloat16
F32 = jnp.float32

SLOT_OF = {0: 0, 1: 1, 7: 2, 2: 3, 6: 4, 3: 5, 5: 6, 4: 7}


def plan(src, dst, send_sem, recv_sem, where):
    return pltpu.make_async_remote_copy(
        src_ref=src,
        dst_ref=dst,
        send_sem=send_sem,
        recv_sem=recv_sem,
        device_id=where,
        device_id_type=MESH_ID,
    )


def send(*args):
    copy = plan(*args)
    copy.start()
    return copy


def mm(a, b):
    return jnp.dot(a, b, preferred_element_type=F32)


def mm_nt(a, b):
    return lax.dot_general(a, b, (((1,), (1,)), ((), ())), preferred_element_type=F32)


def rms_scale(values, gain):
    return values * lax.rsqrt(jnp.mean(values * values, axis=-1, keepdims=True) + EPS) * gain


def events():
    out = []
    z_step, y_step = 7.0 / PARTS, 8.4 / PARTS
    for c in range(CHUNKS):
        at_z = 3 + z_step * (c + 1)
        at_x = at_z + 4
        near = max(at_x + 5, 10.5 + 4 + y_step * c)
        out.append((at_z, 0, "z", c))
        out.append((at_x, 1, "x", c))
        out.append((near, 2, "near", c))
        out.append((near + 3.5, 3, "gate", c))
    last = 0.0
    for s in range(SLOTS):
        ready = max(at for at, _, name, c in out if name == "gate" and c == s * PARTS + PARTS - 1)
        out.append((ready + 0.1, 4, "act", s))
        for h in range(PARTS):
            c = s * PARTS + h
            down = ready + 0.2 + 0.01 * h
            join = max(down + 5, last + y_step)
            done = join + 4
            last = join
            out.append((down, 5, "down", c))
            out.append((join, 6, "join", c))
            out.append((done, 7, "sum", c))
            out.append((done + 4, 8, "back", c))
            out.append((done + 10, 9, "pick", c))
    return [(name, c) for _, _, name, c in sorted(out)]


def layer_kernel(
    latent,
    latent_gain,
    rope_t,
    wide_t,
    narrow_t,
    cosine,
    sine,
    key_wide,
    value_wide,
    key_narrow,
    value_narrow,
    resid,
    attn_gain,
    ffn_gain,
    routes_t,
    logit_t,
    out_wide,
    out_narrow,
    gate_hbm,
    up_hbm,
    down_hbm,
    branch_ref,
    stream_ref,
    qbuf,
    kvbuf,
    w_kv,
    kw_s,
    kn_s,
    vw_s,
    vn_s,
    top_w,
    top_n,
    acc_w,
    acc_n,
    osend,
    orecv,
    ysend,
    yrecv,
    wbuf,
    moe_in,
    sbuf,
    zbuf,
    xsend,
    rows,
    w_in,
    w_out,
    accum,
    hidden,
    pbuf,
    relay,
    ring,
    ebuf,
    xback,
    zsend,
    zback,
    l_sem,
    q_ss,
    q_rs,
    f_ss,
    f_rs,
    b_ss,
    b_rs,
    d_ss,
    d_rs,
    o_ss,
    o_rs,
    h_ss,
    h_rs,
    w_ss,
    w_rs,
    zl_sem,
    z_ss,
    z_rs,
    xl_sem,
    x_ss,
    x_rs,
    y_ss,
    y_rs,
    r_ss,
    r_rs,
    bl_sem,
    bx_ss,
    bx_rs,
    cl_sem,
    bz_ss,
    bz_rs,
):
    z = lax.axis_index("sp_0")
    x = lax.axis_index("sp_1")
    core = lax.axis_index("sp_2")
    y = lax.axis_index("tp")
    zs = {d: lax.rem(z + d, NZ) for d in range(1, NZ)}
    gs = {}
    for dx in range(NX):
        for dc in range(NC):
            if dx or dc:
                gs[dx * NC + dc] = (lax.rem(x + dx, NX), lax.rem(core + dc, NC))
    xs = {j: {"sp_1": lax.rem(x + j, NX)} for j in range(1, NX)}
    ys = {j: {"tp": lax.rem(y + j, NT)} for j in range(1, NT)}
    up, down = {"sp_0": zs[1]}, {"sp_0": zs[7]}
    right, left = ys[1], ys[3]
    sibling = {"sp_2": 1 - core}
    mine = x * NC + core

    peers = [{"sp_0": p} for p in zs.values()]
    peers += [{"sp_1": a, "sp_2": b} for a, b in gs.values()]
    peers += list(ys.values())
    barrier = pltpu.get_barrier_semaphore()
    for peer in peers:
        pl.semaphore_signal(barrier, inc=1, device_id=peer, device_id_type=MESH_ID)

    loads = [
        pltpu.make_async_copy(out_wide, wbuf.at[0, pl.ds(0, 128)], l_sem.at[0]),
        pltpu.make_async_copy(out_narrow, wbuf.at[0, pl.ds(128, 64)], l_sem.at[1]),
        pltpu.make_async_copy(gate_hbm.at[0], w_in.at[:, pl.ds(0, HID)], l_sem.at[2]),
        pltpu.make_async_copy(up_hbm.at[0], w_in.at[:, pl.ds(HID, HID)], l_sem.at[3]),
        pltpu.make_async_copy(down_hbm.at[0], w_out, l_sem.at[4]),
    ]
    for load in loads:
        load.start()

    def turn(values):
        first, second = values[:32].astype(F32), values[32:].astype(F32)
        c, s = cosine[...], sine[...]
        return jnp.concatenate([first * c - second * s, second * c + first * s], axis=0)

    kvbuf[0, 0, :TOK] = rms_scale(latent[...].astype(F32), latent_gain[...]).astype(BF)
    kvbuf[0, 0, TOK:] = turn(rope_t[...]).astype(BF)
    qbuf[0, :, :128] = wide_t[:128].astype(F32).T.astype(BF)
    qbuf[0, :, 128:256] = (
        jnp.concatenate([turn(wide_t[128:]), jnp.zeros((64, TOK), F32)], axis=0).T.astype(BF)
    )
    qbuf[0, :, 256:] = (
        jnp.concatenate([narrow_t[:64].astype(F32), turn(narrow_t[64:])], axis=0).T.astype(BF)
    )

    pl.semaphore_wait(barrier, len(peers))

    half = 160
    fwd, bwd, across = {}, {}, {}

    def at(r):
        return SLOT_OF[r % NZ]

    for k in range(1, 4):
        fwd[k] = plan(
            kvbuf.at[at(k - 1), 0], kvbuf.at[at(k), 0], f_ss.at[k], f_rs.at[k], up
        )
        bwd[k] = plan(
            kvbuf.at[at(1 - k), 0], kvbuf.at[at(-k), 0], b_ss.at[k], b_rs.at[k], down
        )
    first, second = pl.ds(0, half), pl.ds(half, half)
    fwd[4] = plan(
        kvbuf.at[at(3), 0, first], kvbuf.at[at(4), 0, first], f_ss.at[4], f_rs.at[4], up
    )
    bwd[4] = plan(
        kvbuf.at[at(5), 0, second], kvbuf.at[at(4), 0, second], b_ss.at[4], b_rs.at[4], down
    )
    for r in (0, 1, 2, 3, 5, 6, 7):
        across[r] = plan(
            kvbuf.at[at(r), 0], kvbuf.at[at(r), 1], d_ss.at[r], d_rs.at[r], sibling
        )
    across[4] = plan(
        kvbuf.at[at(4), 0, first], kvbuf.at[at(4), 1, first], d_ss.at[4], d_rs.at[4], sibling
    )
    across[8] = plan(
        kvbuf.at[at(4), 0, second], kvbuf.at[at(4), 1, second], d_ss.at[8], d_rs.at[8], sibling
    )
    fwd[1].start()
    bwd[1].start()
    across[0].start()
    qcopies = {
        j: send(qbuf.at[0], qbuf.at[j], q_ss.at[j], q_rs.at[j], xs[j]) for j in (1, 3, 2)
    }
    upper, lower = pl.ds(0, 96), pl.ds(96, 96)
    wcopies = [
        plan(wbuf.at[0], wbuf.at[1], w_ss.at[0], w_rs.at[0], right),
        plan(wbuf.at[0], wbuf.at[3], w_ss.at[1], w_rs.at[1], left),
        plan(wbuf.at[1, upper], wbuf.at[2, upper], w_ss.at[2], w_rs.at[2], right),
        plan(wbuf.at[3, lower], wbuf.at[2, lower], w_ss.at[3], w_rs.at[3], left),
    ]
    loads[0].wait()
    loads[1].wait()
    wcopies[0].start()
    wcopies[1].start()

    lane_w = lax.broadcasted_iota(jnp.int32, (256, 128), 1)
    wide_at = pl.ds(pl.multiple_of(y * 128, 128), 128)
    narrow_at = pl.ds(pl.multiple_of(y // 2 * 128, 128), 128)
    odd = lax.rem(y, 2) == 1

    def narrow(ref):
        both = ref[:, narrow_at].astype(F32)
        return jnp.where(lane_w < 64, jnp.where(odd, pltpu.roll(both, 64, 1), both), 0.0)

    w_kv[:, :128] = key_wide[:, wide_at]
    w_kv[:, 128:256] = narrow(key_narrow).astype(BF)
    w_kv[:, 256:384] = value_wide[:, wide_at]
    w_kv[:, 384:] = narrow(value_narrow).astype(BF)
    vw_s[:, 128:] = jnp.ones((6 * TOK, 128), BF)

    expert = lax.broadcasted_iota(jnp.int32, (SUB, SUB), 0)
    lane = lax.broadcasted_iota(jnp.int32, (SUB, SUB), 1)
    diagonal = expert == lane

    def column(row):
        return jnp.sum(jnp.where(diagonal, row, 0.0), axis=1, keepdims=True)

    chosen = [routes_t[k : k + 1, :] for k in range(2)]
    named = [(expert == row).astype(F32) for row in chosen]
    earlier = (expert < lane).astype(BF)
    before = mm((named[0] + named[1]).astype(BF), earlier)
    slots = [jnp.sum(before * one, axis=0, keepdims=True) for one in named]
    named_here = [(column(row.astype(F32)) == lane.astype(F32)) for row in chosen]
    slots_here = [column(row) for row in slots]

    def placing(s):
        return jnp.where(slots[0] == s, named[0], 0.0) + jnp.where(slots[1] == s, named[1], 0.0)

    def picking(k, s):
        return jnp.where(named_here[k] & (slots_here[k] == s), 1.0, 0.0).astype(BF)

    logits = [logit_t[k : k + 1, :] for k in range(2)]
    peak = jnp.maximum(logits[0], logits[1])
    parts = [jnp.exp(row - peak) for row in logits]
    share = [column(part / (parts[0] + parts[1])) for part in parts]
    order = (expert // NZ == lax.rem(lane, GROUP)) & (lax.rem(expert, NZ) == lane // GROUP)
    order_back = (expert // GROUP == lax.rem(lane, NZ)) & (lax.rem(expert, GROUP) == lane // NZ)
    order = order.astype(F32).astype(BF)
    order_back = order_back.astype(F32).astype(BF)

    lane_q = lax.broadcasted_iota(jnp.int32, (TOK, 128), 1)

    def expand(base, count):
        def one(i, carry):
            piece = kvbuf[base + i // NC, lax.rem(i, NC)]
            to = pl.ds(pl.multiple_of(i * TOK, TOK), TOK)
            full = mm(piece[:TOK], w_kv[...])
            turned = piece[TOK:].astype(F32)
            tail = jnp.concatenate([turned, turned], axis=0).T
            kw_s[to, :128] = full[:, :128].astype(BF)
            kw_s[to, 128:] = tail.astype(BF)
            kn_s[to] = jnp.where(lane_q < 64, full[:, 128:256], tail).astype(BF)
            vw_s[to, :128] = full[:, 256:384].astype(BF)
            vn_s[to] = jnp.where(lane_q < 64, full[:, 384:], 1.0).astype(BF)
            return carry

        lax.fori_loop(0, count * NC, one, 0)

    def one_head(q, keys, values, top, acc, j, factor, fresh):
        scores = mm_nt(q, keys)
        best = jnp.max(scores, axis=1, keepdims=True)
        if fresh:
            new = jnp.broadcast_to(best, (TOK, 128))
        else:
            old = top[j]
            new = jnp.maximum(old, best)
            shrink = jnp.exp2((old - new) * factor)
            best = new[:, :1]
        weights = jnp.exp2((scores - best) * factor).astype(BF)
        summed = mm(weights, values)
        if not fresh:
            wide = shrink if summed.shape[1] == 128 else jnp.concatenate([shrink, shrink], axis=1)
            summed = acc[j] * wide + summed
        acc[j] = summed
        top[j] = new

    def attend(j, count, fresh):
        keys = count * NC * TOK
        q = qbuf[j]
        one_head(q[:, :256], kw_s[:keys], vw_s[:keys], top_w, acc_w, j, FACTOR_W, fresh)
        one_head(q[:, 256:], kn_s[:keys], vn_s[:keys], top_n, acc_n, j, FACTOR_N, fresh)

    def forward(k):
        fwd[k].wait_recv()
        fwd[k + 1].start()
        across[k].start()
        bwd[k].wait_recv()
        bwd[k + 1].start()
        across[NZ - k].start()

    forward(1)
    for r in (0, 1, 7):
        across[r].wait_recv()
    expand(0, 3)

    def first_body(j, carry):
        for other in range(1, NX):

            @pl.when(j == other)
            def _():
                qcopies[other].wait_recv()

        attend(j, 3, True)

        @pl.when(j == 1)
        def _():
            forward(2)

        return carry

    lax.fori_loop(0, NX, first_body, 0)
    for r in (2, 6):
        across[r].wait_recv()
    expand(3, 2)

    def second_body(j, carry):
        attend(j, 2, False)

        @pl.when(j == 1)
        def _():
            forward(3)
            wcopies[0].wait_recv()
            wcopies[2].start()
            wcopies[1].wait_recv()
            wcopies[3].start()

        return carry

    lax.fori_loop(0, NX, second_body, 0)
    fwd[4].wait_recv()
    across[4].start()
    bwd[4].wait_recv()
    across[8].start()
    for r in (3, 5, 4, 8):
        across[r].wait_recv()
    expand(5, 3)

    def three(value):
        high = value.astype(BF).astype(F32)
        rest = value - high
        middle = rest.astype(BF).astype(F32)
        return high, middle, rest - middle

    def finish(j):
        total_w = acc_w[j, :, 128:]
        osend[j, :, :128] = (acc_w[j, :, :128] / total_w).astype(BF)
        both = acc_n[j]
        tail = both / pltpu.roll(both, 64, 1)
        level_w = top_w[j] * FACTOR_W + jnp.log2(total_w)
        level_n = top_n[j] * FACTOR_N + jnp.log2(both)
        at_lane = 64
        for part in three(level_w) + three(level_n):
            tail = jnp.where(lane_q == at_lane, part, tail)
            at_lane += 1
        osend[j, :, 128:] = tail.astype(BF)

    ocopies = {
        j: plan(osend.at[j], orecv.at[j], o_ss.at[j], o_rs.at[j], xs[NX - j]) for j in (1, 2, 3)
    }

    def last_body(i, carry):
        j = NX - 1 - i
        attend(j, 3, False)
        finish(j)
        for other in range(1, NX):

            @pl.when(j == other)
            def _():
                ocopies[other].start()

        return carry

    lax.fori_loop(0, NX, last_body, 0)
    for j in (3, 2, 1):
        ocopies[j].wait_recv()

    tails = [osend[0, :, 128:].astype(F32)] + [orecv[j, :, 128:].astype(F32) for j in (1, 2, 3)]
    mains = [osend[0, :, :128]] + [orecv[j, :, :128] for j in (1, 2, 3)]

    def weigh(a):
        levels = [(t[:, a : a + 1] + t[:, a + 1 : a + 2]) + t[:, a + 2 : a + 3] for t in tails]
        best = functools.reduce(jnp.maximum, levels)
        portions = [jnp.exp2(level - best) for level in levels]
        total = functools.reduce(jnp.add, portions)
        return [portion / total for portion in portions]

    merged_w = functools.reduce(jnp.add, [m.astype(F32) * s for m, s in zip(mains, weigh(64))])
    merged_n = functools.reduce(jnp.add, [t * s for t, s in zip(tails, weigh(67))])
    ysend[:, :128] = merged_w.astype(BF)
    ysend[:, 128:] = jnp.where(lane_q < 64, merged_n, 0.0).astype(BF)
    hcopies = {}
    for j in (2, 1, 3):
        part = pl.ds(pl.multiple_of(lax.rem(y + j, NT) * SUB, SUB), SUB)
        hcopies[j] = send(ysend.at[part], yrecv.at[j], h_ss.at[j], h_rs.at[j], ys[j])

    own = ysend[pl.ds(pl.multiple_of(y * SUB, SUB), SUB)]
    proj = mm(own[:, :192], wbuf[0]).astype(BF).astype(F32)
    for j, needed in ((1, (0,)), (3, (1,)), (2, (2, 3))):
        if j == 2:
            for copy in needed:
                wcopies[copy].wait_recv()
        hcopies[j].wait_recv()
        proj = proj + mm(yrecv[j, :, :192], wbuf[j]).astype(BF).astype(F32)
    stream = (resid[...].astype(F32) + rms_scale(proj, attn_gain[...])).astype(BF)
    stream_ref[...] = stream
    moe_in[...] = rms_scale(stream.astype(F32), ffn_gain[...]).astype(BF)

    z_order = (4, 3, 5, 2, 6, 1, 7)
    x_order = (4, 5, 2, 3, 6, 7, 1)

    def seg(number):
        return pl.ds(pl.multiple_of(number * 8, 8), 8)

    def over_z(src, dst, c, local_sem, ss, rs):
        copies = {
            d: send(
                src.at[c, seg(zs[d])],
                dst.at[c, seg(z)],
                ss.at[c, d],
                rs.at[c, d],
                {"sp_0": zs[d]},
            )
            for d in z_order
        }
        kept = pltpu.make_async_copy(src.at[c, seg(z)], dst.at[c, seg(z)], local_sem.at[c])
        kept.start()
        return copies, kept

    def over_x(src, dst, c, local_sem, ss, rs):
        copies = {}
        for d in x_order:
            a, b = gs[d]
            copies[d] = send(
                src(c, seg(a * NC + b)),
                dst(c, seg(mine)),
                ss.at[c, d],
                rs.at[c, d],
                {"sp_1": a, "sp_2": b},
            )
        kept = pltpu.make_async_copy(src(c, seg(mine)), dst(c, seg(mine)), local_sem.at[c])
        kept.start()
        return copies, kept

    def arrived(moved):
        copies, kept = moved
        kept.wait()
        for copy in copies.values():
            copy.wait_recv()

    def lanes(c):
        h = c % PARTS
        return slice(h * LANES, (h + 1) * LANES)

    z_moves, x_moves, near, far = {}, {}, {}, {}
    sums, joined, back_x, back_z = {}, {}, {}, {}
    high, low = pl.ds(0, HALF), pl.ds(HALF, HALF)

    for s in range(SLOTS):
        place = placing(s).astype(BF)
        for h in range(PARTS):
            c = s * PARTS + h
            sbuf[c] = mm(place, moe_in[:, lanes(c)]).astype(BF)
            z_moves[c] = over_z(sbuf, zbuf, c, zl_sem, z_ss, z_rs)

    def stage_z(c):
        arrived(z_moves[c])
        xsend[c] = mm(order, zbuf[c]).astype(BF)
        x_moves[c] = over_x(
            lambda c, s: xsend.at[c, s], lambda c, s: rows.at[c, 0, s], c, xl_sem, x_ss, x_rs
        )

    def stage_x(c):
        arrived(x_moves[c])
        near[c] = (
            send(rows.at[c, 0], rows.at[c, 1], y_ss.at[c, 0], y_rs.at[c, 0], right),
            send(rows.at[c, 0], rows.at[c, 3], y_ss.at[c, 1], y_rs.at[c, 1], left),
        )

    def stage_near(c):
        near[c][0].wait_recv()
        one = send(rows.at[c, 1, high], rows.at[c, 2, high], y_ss.at[c, 2], y_rs.at[c, 2], right)
        near[c][1].wait_recv()
        two = send(rows.at[c, 3, low], rows.at[c, 2, low], y_ss.at[c, 3], y_rs.at[c, 3], left)
        far[c] = (one, two)

    def stage_gate(c):
        for copy in far[c]:
            copy.wait_recv()
        if c == 0:
            loads[2].wait()
            loads[3].wait()

        def tile(n, carry):
            to = pl.ds(pl.multiple_of(n * 256, 256), 256)
            part = mm(rows[c].reshape(NT * ROWS, LANES), w_in[lanes(c), to])
            if c % PARTS == 0:
                accum[:, to] = part
            else:
                accum[:, to] += part
            return carry

        lax.fori_loop(0, 2 * HID // 256, tile, 0)

    def stage_act(s):
        def some(b, carry):
            part = pl.ds(pl.multiple_of(b * 64, 64), 64)
            hidden[part] = (jax.nn.silu(accum[part, :HID]) * accum[part, HID:]).astype(BF)
            return carry

        lax.fori_loop(0, NT * ROWS // 64, some, 0)
        if s == 0:
            loads[4].wait()

    def stage_down(c):
        def tile(n, carry):
            to = pl.ds(pl.multiple_of(n * 256, 256), 256)
            at_lane = pl.ds(pl.multiple_of(c % PARTS * LANES + n * 256, 256), 256)
            part = mm(hidden[...], w_out[:, at_lane]).astype(BF)
            pbuf[c, :, :, to] = part.reshape(NT, ROWS, 256)
            return carry

        lax.fori_loop(0, LANES // 256, tile, 0)
        sums[c] = [
            send(pbuf.at[c, 2, high], relay.at[c, 0], r_ss.at[c, 0], r_rs.at[c, 0], right),
            send(pbuf.at[c, 2, low], relay.at[c, 1], r_ss.at[c, 1], r_rs.at[c, 1], left),
            send(pbuf.at[c, 3, low], ring.at[c, 0, low], r_ss.at[c, 2], r_rs.at[c, 2], right),
            send(pbuf.at[c, 1, high], ring.at[c, 1, high], r_ss.at[c, 3], r_rs.at[c, 3], left),
        ]

    def stage_join(c):
        sums[c][0].wait_recv()
        pbuf[c, 3, :HALF] = (
            pbuf[c, 3, :HALF].astype(F32) + relay[c, 0].astype(F32)
        ).astype(BF)
        one = send(pbuf.at[c, 3, high], ring.at[c, 0, high], r_ss.at[c, 4], r_rs.at[c, 4], right)
        sums[c][1].wait_recv()
        pbuf[c, 1, HALF:] = (
            pbuf[c, 1, HALF:].astype(F32) + relay[c, 1].astype(F32)
        ).astype(BF)
        two = send(pbuf.at[c, 1, low], ring.at[c, 1, low], r_ss.at[c, 5], r_rs.at[c, 5], left)
        joined[c] = (one, two)

    def stage_sum(c):
        for copy in sums[c][2:] + list(joined[c]):
            copy.wait_recv()
        ebuf[c] = (
            pbuf[c, 0].astype(F32) + ring[c, 0].astype(F32) + ring[c, 1].astype(F32)
        ).astype(BF)
        back_x[c] = over_x(
            lambda c, s: ebuf.at[c, s], lambda c, s: xback.at[c, s], c, bl_sem, bx_ss, bx_rs
        )

    def stage_back(c):
        arrived(back_x[c])
        zsend[c] = mm(order_back, xback[c]).astype(BF)
        back_z[c] = over_z(zsend, zback, c, cl_sem, bz_ss, bz_rs)

    def stage_pick(c):
        arrived(back_z[c])
        s = c // PARTS
        part = share[0] * mm(picking(0, s), zback[c]) + share[1] * mm(picking(1, s), zback[c])
        if s == 0:
            branch_ref[:, lanes(c)] = part
        else:
            branch_ref[:, lanes(c)] += part

    stages = {
        "z": stage_z,
        "x": stage_x,
        "near": stage_near,
        "gate": stage_gate,
        "act": stage_act,
        "down": stage_down,
        "join": stage_join,
        "sum": stage_sum,
        "back": stage_back,
        "pick": stage_pick,
    }
    for name, c in events():
        stages[name](c)

    for moves in (z_moves, x_moves, back_x, back_z):
        for copies, _ in moves.values():
            for copy in copies.values():
                copy.wait_send()
    for group in (near, far, sums, joined):
        for copies in group.values():
            for copy in copies:
                copy.wait_send()
    for group in (fwd, bwd, across, qcopies, ocopies, hcopies):
        for copy in group.values():
            copy.wait_send()
    for copy in wcopies:
        copy.wait_send()


def layer(*args):
    dma = pltpu.SemaphoreType.DMA
    vmem = pl.BlockSpec(memory_space=pltpu.VMEM)
    hbm = pl.BlockSpec(memory_space=pl.ANY)
    buf = pltpu.VMEM((CHUNKS, ROWS, LANES), BF)
    return pl.pallas_call(
        layer_kernel,
        out_shape=(
            jax.ShapeDtypeStruct((SUB, D), F32),
            jax.ShapeDtypeStruct((SUB, D), BF),
        ),
        in_specs=[vmem] * 16 + [hbm] * 5,
        out_specs=(vmem, vmem),
        scratch_shapes=[
            pltpu.VMEM((NX, TOK, 384), BF),
            pltpu.VMEM((NZ, NC, TOK + ROPE, 256), BF),
            pltpu.VMEM((256, 512), BF),
            pltpu.VMEM((6 * TOK, 256), BF),
            pltpu.VMEM((6 * TOK, 128), BF),
            pltpu.VMEM((6 * TOK, 256), BF),
            pltpu.VMEM((6 * TOK, 128), BF),
            pltpu.VMEM((NX, TOK, 128), F32),
            pltpu.VMEM((NX, TOK, 128), F32),
            pltpu.VMEM((NX, TOK, 256), F32),
            pltpu.VMEM((NX, TOK, 128), F32),
            pltpu.VMEM((NX, TOK, 256), BF),
            pltpu.VMEM((NX, TOK, 256), BF),
            pltpu.VMEM((TOK, 256), BF),
            pltpu.VMEM((NT, SUB, 256), BF),
            pltpu.VMEM((NT, 192, D), BF),
            pltpu.VMEM((SUB, D), BF),
            buf,
            buf,
            buf,
            pltpu.VMEM((CHUNKS, NT, ROWS, LANES), BF),
            pltpu.VMEM((D, 2 * HID), BF),
            pltpu.VMEM((HID, D), BF),
            pltpu.VMEM((NT * ROWS, 2 * HID), F32),
            pltpu.VMEM((NT * ROWS, HID), BF),
            pltpu.VMEM((CHUNKS, NT, ROWS, LANES), BF),
            pltpu.VMEM((CHUNKS, 2, HALF, LANES), BF),
            pltpu.VMEM((CHUNKS, 2, ROWS, LANES), BF),
            buf,
            buf,
            buf,
            buf,
            dma((5,)),
            dma((NX,)),
            dma((NX,)),
            dma((5,)),
            dma((5,)),
            dma((5,)),
            dma((5,)),
            dma((9,)),
            dma((9,)),
            dma((NX,)),
            dma((NX,)),
            dma((NT,)),
            dma((NT,)),
            dma((4,)),
            dma((4,)),
            dma((CHUNKS,)),
            dma((CHUNKS, NZ)),
            dma((CHUNKS, NZ)),
            dma((CHUNKS,)),
            dma((CHUNKS, GROUP)),
            dma((CHUNKS, GROUP)),
            dma((CHUNKS, 4)),
            dma((CHUNKS, 4)),
            dma((CHUNKS, 6)),
            dma((CHUNKS, 6)),
            dma((CHUNKS,)),
            dma((CHUNKS, GROUP)),
            dma((CHUNKS, GROUP)),
            dma((CHUNKS,)),
            dma((CHUNKS, NZ)),
            dma((CHUNKS, NZ)),
        ],
        compiler_params=pltpu.CompilerParams(
            collective_id=0, has_side_effects=True, vmem_limit_bytes=58 * 1024 * 1024
        ),
        name="layer",
    )(*args)


def local(
    resid,
    query_wide,
    query_narrow,
    latent,
    rope_key,
    latent_gain,
    key_up_wide,
    value_up_wide,
    key_up_narrow,
    value_up_narrow,
    out_wide,
    out_narrow,
    attn_gain,
    ffn_gain,
    moe_gain,
    routes,
    route_logit,
    expert_gate,
    expert_up,
    expert_down,
):
    positions = lax.axis_index(SP) * TOK + jnp.arange(TOK, dtype=jnp.int32)
    freq = THETA ** (-jnp.arange(ROPE // 2, dtype=jnp.float32) * 2.0 / ROPE)
    angle = freq[:, None] * positions.astype(jnp.float32)[None, :]
    branch, stream = layer(
        latent,
        latent_gain[None],
        rope_key.T,
        query_wide.T,
        query_narrow.T,
        jnp.cos(angle),
        jnp.sin(angle),
        key_up_wide,
        value_up_wide,
        key_up_narrow,
        value_up_narrow,
        resid,
        attn_gain[None],
        ffn_gain[None],
        routes.T,
        route_logit.T,
        out_wide,
        out_narrow,
        expert_gate,
        expert_up,
        expert_down,
    )
    return (stream.astype(jnp.float32) + rms_scale(branch, moe_gain)).astype(jnp.bfloat16)


def solution(mesh):
    split = Mesh(mesh.devices.reshape(8, 4, 2, mesh.shape["tp"]), ("sp_0", "sp_1", "sp_2", "tp"))
    in_specs = (
        P(SP_TP, None),
        P(SP, "tp"),
        P(SP, "tp"),
        P(SP, None),
        P(SP, None),
        P(),
        P(),
        P(),
        P(),
        P(),
        P("tp", None),
        P("tp", None),
        P(),
        P(),
        P(),
        P(SP_TP, None),
        P(SP_TP, None),
        P(SP, None, "tp"),
        P(SP, None, "tp"),
        P(SP, "tp", None),
    )
    out_specs = P(SP_TP, None)
    return jax.shard_map(local, mesh=split, in_specs=in_specs, out_specs=out_specs, check_vma=False)
```

```python
import functools
import math

import jax
import jax.numpy as jnp
from jax import lax
from jax.experimental import pallas as pl
from jax.experimental.pallas import tpu as pltpu
from jax.sharding import Mesh
from jax.sharding import PartitionSpec as P

NOPE_W = 128
NOPE_N = 64
ROPE = 64
SP = ("sp_0", "sp_1", "sp_2")
SP_TP = ("sp_0", "sp_1", "sp_2", "tp")
NZ, NX, NC, NT = 8, 4, 2, 4
TOK = 256
SUB = 64
D = 2048
LOG2E = math.log2(math.e)
MESH_ID = pl.DeviceIdType.MESH

EPS = 1e-06
THETA = 10000.0

GROUP = NX * NC
SLOTS = 3
PARTS = 2
LANES = D // PARTS
CHUNKS = SLOTS * PARTS
ROWS = NZ * GROUP
HID = 896
HALF = ROWS // 2

FACTOR_W = (NOPE_W + ROPE) ** (-0.5) * LOG2E
FACTOR_N = (NOPE_N + ROPE) ** (-0.5) * LOG2E

BF = jnp.bfloat16
F32 = jnp.float32

SLOT_OF = {0: 0, 1: 1, 7: 2, 2: 3, 6: 4, 3: 5, 5: 6, 4: 7}


def plan(src, dst, send_sem, recv_sem, where):
    return pltpu.make_async_remote_copy(
        src_ref=src,
        dst_ref=dst,
        send_sem=send_sem,
        recv_sem=recv_sem,
        device_id=where,
        device_id_type=MESH_ID,
    )


def send(*args):
    copy = plan(*args)
    copy.start()
    return copy


def mm(a, b):
    return jnp.dot(a, b, preferred_element_type=F32)


def mm_nt(a, b):
    return lax.dot_general(a, b, (((1,), (1,)), ((), ())), preferred_element_type=F32)


def rms_scale(values, gain):
    return values * lax.rsqrt(jnp.mean(values * values, axis=-1, keepdims=True) + EPS) * gain


STAGES = (
    "z0 z1 x0 z2",
    "x1 z3 near0 x2",
    "z4 near1 x3 gate0",
    "z5 x4 near2 gate1",
    "act0 down0 near3 x5",
    "down1 near4 gate2 join0",
    "near5 gate3 act1 down2",
    "join1 down3 gate4 sum0",
    "join2 gate5 join3 back0",
    "act2 down4 down5 sum1",
    "sum2 sum3 pick0 join4",
    "back1 back2 join5 back3",
    "sum4 pick1 sum5 pick2",
    "back4 back5 pick3 pick4",
    "pick5",
)


def layer_kernel(
    latent,
    latent_gain,
    rope_t,
    wide_t,
    narrow_q,
    cosine,
    sine,
    key_wide,
    value_wide,
    key_narrow,
    value_narrow,
    resid,
    attn_gain,
    ffn_gain,
    moe_gain,
    routes_t,
    logit_t,
    out_wide,
    out_narrow,
    gate_hbm,
    up_hbm,
    down_hbm,
    mixed_ref,
    branch_ref,
    qbuf,
    kvbuf,
    w_kv,
    kw_s,
    kn_s,
    vw_s,
    vn_s,
    top_w,
    top_n,
    acc_w,
    acc_n,
    osend,
    orecv,
    ysend,
    yrecv,
    wbuf,
    moe_in,
    sbuf,
    zbuf,
    xsend,
    rows,
    w_in,
    w_out,
    accum,
    hidden,
    pbuf,
    relay,
    ring,
    ebuf,
    xback,
    zsend,
    zback,
    l_sem,
    q_ss,
    q_rs,
    f_ss,
    f_rs,
    b_ss,
    b_rs,
    d_ss,
    d_rs,
    o_ss,
    o_rs,
    h_ss,
    h_rs,
    w_ss,
    w_rs,
    zl_sem,
    z_ss,
    z_rs,
    xl_sem,
    x_ss,
    x_rs,
    y_ss,
    y_rs,
    r_ss,
    r_rs,
    bl_sem,
    bx_ss,
    bx_rs,
    cl_sem,
    bz_ss,
    bz_rs,
):
    z = lax.axis_index("sp_0")
    x = lax.axis_index("sp_1")
    core = lax.axis_index("sp_2")
    y = lax.axis_index("tp")
    zs = {d: lax.rem(z + d, NZ) for d in range(1, NZ)}
    gs = {}
    for dx in range(NX):
        for dc in range(NC):
            if dx or dc:
                gs[dx * NC + dc] = (lax.rem(x + dx, NX), lax.rem(core + dc, NC))
    xs = {j: {"sp_1": lax.rem(x + j, NX)} for j in range(1, NX)}
    ys = {j: {"tp": lax.rem(y + j, NT)} for j in range(1, NT)}
    up, down = {"sp_0": zs[1]}, {"sp_0": zs[7]}
    right, left = ys[1], ys[3]
    sibling = {"sp_2": 1 - core}
    mine = x * NC + core

    peers = [{"sp_0": p} for p in zs.values()]
    peers += [{"sp_1": a, "sp_2": b} for a, b in gs.values()]
    peers += list(ys.values())
    barrier = pltpu.get_barrier_semaphore()
    for peer in peers:
        pl.semaphore_signal(barrier, inc=1, device_id=peer, device_id_type=MESH_ID)

    loads = [
        pltpu.make_async_copy(out_wide, wbuf.at[0, pl.ds(0, 128)], l_sem.at[0]),
        pltpu.make_async_copy(out_narrow, wbuf.at[0, pl.ds(128, 64)], l_sem.at[1]),
        pltpu.make_async_copy(gate_hbm.at[0], w_in.at[:, pl.ds(0, HID)], l_sem.at[2]),
        pltpu.make_async_copy(up_hbm.at[0], w_in.at[:, pl.ds(HID, HID)], l_sem.at[3]),
        pltpu.make_async_copy(down_hbm.at[0], w_out, l_sem.at[4]),
    ]
    for load in loads:
        load.start()

    def turn(values):
        first, second = values[:32].astype(F32), values[32:].astype(F32)
        c, s = cosine[...], sine[...]
        return jnp.concatenate([first * c - second * s, second * c + first * s], axis=0)

    kvbuf[0, 0, :TOK] = rms_scale(latent[...].astype(F32), latent_gain[...]).astype(BF)
    kvbuf[0, 0, TOK:] = turn(rope_t[...]).astype(BF)
    narrow_t = narrow_q[...].astype(F32).T
    qbuf[0, :, :128] = wide_t[:128].astype(F32).T.astype(BF)
    qbuf[0, :, 128:256] = (
        jnp.concatenate([turn(wide_t[128:]), jnp.zeros((64, TOK), F32)], axis=0).T.astype(BF)
    )
    qbuf[0, :, 256:] = (
        jnp.concatenate([narrow_t[:64], turn(narrow_t[64:])], axis=0).T.astype(BF)
    )

    pl.semaphore_wait(barrier, len(peers))

    half = 160
    fwd, bwd, across = {}, {}, {}

    def at(r):
        return SLOT_OF[r % NZ]

    for k in range(1, 4):
        fwd[k] = plan(
            kvbuf.at[at(k - 1), 0], kvbuf.at[at(k), 0], f_ss.at[k], f_rs.at[k], up
        )
        bwd[k] = plan(
            kvbuf.at[at(1 - k), 0], kvbuf.at[at(-k), 0], b_ss.at[k], b_rs.at[k], down
        )
    first, second = pl.ds(0, half), pl.ds(half, half)
    fwd[4] = plan(
        kvbuf.at[at(3), 0, first], kvbuf.at[at(4), 0, first], f_ss.at[4], f_rs.at[4], up
    )
    bwd[4] = plan(
        kvbuf.at[at(5), 0, second], kvbuf.at[at(4), 0, second], b_ss.at[4], b_rs.at[4], down
    )
    for r in (0, 1, 2, 3, 5, 6, 7):
        across[r] = plan(
            kvbuf.at[at(r), 0], kvbuf.at[at(r), 1], d_ss.at[r], d_rs.at[r], sibling
        )
    across[4] = plan(
        kvbuf.at[at(4), 0, first], kvbuf.at[at(4), 1, first], d_ss.at[4], d_rs.at[4], sibling
    )
    across[8] = plan(
        kvbuf.at[at(4), 0, second], kvbuf.at[at(4), 1, second], d_ss.at[8], d_rs.at[8], sibling
    )
    fwd[1].start()
    bwd[1].start()
    across[0].start()
    qcopies = {
        j: send(qbuf.at[0], qbuf.at[j], q_ss.at[j], q_rs.at[j], xs[j]) for j in (1, 3, 2)
    }
    upper, lower = pl.ds(0, 96), pl.ds(96, 96)
    wcopies = [
        plan(wbuf.at[0], wbuf.at[1], w_ss.at[0], w_rs.at[0], right),
        plan(wbuf.at[0], wbuf.at[3], w_ss.at[1], w_rs.at[1], left),
        plan(wbuf.at[1, upper], wbuf.at[2, upper], w_ss.at[2], w_rs.at[2], right),
        plan(wbuf.at[3, lower], wbuf.at[2, lower], w_ss.at[3], w_rs.at[3], left),
    ]
    loads[0].wait()
    loads[1].wait()
    wcopies[0].start()
    wcopies[1].start()

    lane_w = lax.broadcasted_iota(jnp.int32, (256, 128), 1)
    wide_at = pl.ds(pl.multiple_of(y * 128, 128), 128)
    narrow_at = pl.ds(pl.multiple_of(y // 2 * 128, 128), 128)
    odd = lax.rem(y, 2) == 1

    def narrow(ref):
        both = ref[:, narrow_at].astype(F32)
        return jnp.where(lane_w < 64, jnp.where(odd, pltpu.roll(both, 64, 1), both), 0.0)

    w_kv[:, :128] = key_wide[:, wide_at]
    w_kv[:, 128:256] = narrow(key_narrow).astype(BF)
    w_kv[:, 256:384] = value_wide[:, wide_at]
    w_kv[:, 384:] = narrow(value_narrow).astype(BF)
    vw_s[:, 128:] = jnp.ones((6 * TOK, 128), BF)

    expert = lax.broadcasted_iota(jnp.int32, (SUB, SUB), 0)
    lane = lax.broadcasted_iota(jnp.int32, (SUB, SUB), 1)
    diagonal = expert == lane

    def column(row):
        return jnp.sum(jnp.where(diagonal, row, 0.0), axis=1, keepdims=True)

    chosen = [routes_t[k : k + 1, :] for k in range(2)]
    named = [(expert == row).astype(F32) for row in chosen]
    earlier = (expert < lane).astype(BF)
    before = mm((named[0] + named[1]).astype(BF), earlier)
    slots = [jnp.sum(before * one, axis=0, keepdims=True) for one in named]
    named_here = [(column(row.astype(F32)) == lane.astype(F32)) for row in chosen]
    slots_here = [column(row) for row in slots]

    def placing(s):
        return jnp.where(slots[0] == s, named[0], 0.0) + jnp.where(slots[1] == s, named[1], 0.0)

    def picking(k, s):
        return jnp.where(named_here[k] & (slots_here[k] == s), 1.0, 0.0).astype(BF)

    logits = [logit_t[k : k + 1, :] for k in range(2)]
    peak = jnp.maximum(logits[0], logits[1])
    parts = [jnp.exp(row - peak) for row in logits]
    share = [column(part / (parts[0] + parts[1])) for part in parts]
    order = (expert // NZ == lax.rem(lane, GROUP)) & (lax.rem(expert, NZ) == lane // GROUP)
    order_back = (expert // GROUP == lax.rem(lane, NZ)) & (lax.rem(expert, GROUP) == lane // NZ)
    order = order.astype(F32).astype(BF)
    order_back = order_back.astype(F32).astype(BF)

    lane_q = lax.broadcasted_iota(jnp.int32, (TOK, 128), 1)

    def expand(base, begin, end):
        def one(i, carry):
            piece = kvbuf[base + i // NC, lax.rem(i, NC)]
            to = pl.ds(pl.multiple_of(i * TOK, TOK), TOK)
            full = mm(piece[:TOK], w_kv[...])
            turned = piece[TOK:].astype(F32)
            tail = jnp.concatenate([turned, turned], axis=0).T
            kw_s[to, :128] = full[:, :128].astype(BF)
            kw_s[to, 128:] = tail.astype(BF)
            kn_s[to] = jnp.where(lane_q < 64, full[:, 128:256], tail).astype(BF)
            vw_s[to, :128] = full[:, 256:384].astype(BF)
            vn_s[to] = jnp.where(lane_q < 64, full[:, 384:], 1.0).astype(BF)
            return carry

        lax.fori_loop(begin, end, one, 0)

    def one_head(q, keys, values, top, acc, j, factor, fresh):
        scores = mm_nt(q, keys)
        best = jnp.max(scores, axis=1, keepdims=True)
        if fresh:
            new = jnp.broadcast_to(best, (TOK, 128))
        else:
            old = top[j]
            new = jnp.maximum(old, best)
            shrink = jnp.exp2((old - new) * factor)
            best = new[:, :1]
        weights = jnp.exp2((scores - best) * factor).astype(BF)
        summed = mm(weights, values)
        if not fresh:
            wide = shrink if summed.shape[1] == 128 else jnp.concatenate([shrink, shrink], axis=1)
            summed = acc[j] * wide + summed
        acc[j] = summed
        top[j] = new

    def attend(j, count, fresh):
        keys = count * NC * TOK
        q = qbuf[j]
        one_head(q[:, :256], kw_s[:keys], vw_s[:keys], top_w, acc_w, j, FACTOR_W, fresh)
        one_head(q[:, 256:], kn_s[:keys], vn_s[:keys], top_n, acc_n, j, FACTOR_N, fresh)

    def forward(k):
        fwd[k].wait_recv()
        fwd[k + 1].start()
        across[k].start()
        bwd[k].wait_recv()
        bwd[k + 1].start()
        across[NZ - k].start()

    expand(0, 0, 1)
    across[0].wait_recv()
    expand(0, 1, 2)
    forward(1)
    expand(0, 2, 3)
    across[1].wait_recv()
    expand(0, 3, 5)
    across[7].wait_recv()
    expand(0, 5, 6)

    def first_body(j, carry):
        for other in range(1, NX):

            @pl.when(j == other)
            def _():
                qcopies[other].wait_recv()

        attend(j, 3, True)

        @pl.when(j == 1)
        def _():
            forward(2)

        return carry

    lax.fori_loop(0, NX, first_body, 0)
    for r in (2, 6):
        across[r].wait_recv()
    expand(3, 0, 4)

    def second_body(j, carry):
        attend(j, 2, False)

        @pl.when(j == 1)
        def _():
            forward(3)
            wcopies[0].wait_recv()
            wcopies[2].start()
            wcopies[1].wait_recv()
            wcopies[3].start()

        return carry

    lax.fori_loop(0, NX, second_body, 0)
    fwd[4].wait_recv()
    across[4].start()
    bwd[4].wait_recv()
    across[8].start()
    for r in (3, 5, 4, 8):
        across[r].wait_recv()
    expand(5, 0, 6)

    def three(value):
        high = value.astype(BF).astype(F32)
        rest = value - high
        middle = rest.astype(BF).astype(F32)
        return high, middle, rest - middle

    def finish(j):
        total_w = acc_w[j, :, 128:]
        osend[j, :, :128] = (acc_w[j, :, :128] / total_w).astype(BF)
        both = acc_n[j]
        tail = both / pltpu.roll(both, 64, 1)
        level_w = top_w[j] * FACTOR_W + jnp.log2(total_w)
        level_n = top_n[j] * FACTOR_N + jnp.log2(both)
        at_lane = 64
        for part in three(level_w) + three(level_n):
            tail = jnp.where(lane_q == at_lane, part, tail)
            at_lane += 1
        osend[j, :, 128:] = tail.astype(BF)

    ocopies = {
        j: plan(osend.at[j], orecv.at[j], o_ss.at[j], o_rs.at[j], xs[NX - j]) for j in (1, 2, 3)
    }

    def last_body(i, carry):
        j = 2 + i - i // 2 * (2 * i - 1)
        attend(j, 3, False)
        finish(j)
        for other in range(1, NX):

            @pl.when(j == other)
            def _():
                ocopies[other].start()

        return carry

    lax.fori_loop(0, NX, last_body, 0)
    for j in (2, 3, 1):
        ocopies[j].wait_recv()

    tails = [osend[0, :, 128:].astype(F32)] + [orecv[j, :, 128:].astype(F32) for j in (1, 2, 3)]
    mains = [osend[0, :, :128]] + [orecv[j, :, :128] for j in (1, 2, 3)]

    def weigh(a):
        levels = [(t[:, a : a + 1] + t[:, a + 1 : a + 2]) + t[:, a + 2 : a + 3] for t in tails]
        best = functools.reduce(jnp.maximum, levels)
        portions = [jnp.exp2(level - best) for level in levels]
        total = functools.reduce(jnp.add, portions)
        return [portion / total for portion in portions]

    merged_w = functools.reduce(jnp.add, [m.astype(F32) * s for m, s in zip(mains, weigh(64))])
    merged_n = functools.reduce(jnp.add, [t * s for t, s in zip(tails, weigh(67))])
    ysend[:, :128] = merged_w.astype(BF)
    ysend[:, 128:] = jnp.where(lane_q < 64, merged_n, 0.0).astype(BF)
    hcopies = {}
    for j in (2, 1, 3):
        part = pl.ds(pl.multiple_of(lax.rem(y + j, NT) * SUB, SUB), SUB)
        hcopies[j] = send(ysend.at[part], yrecv.at[j], h_ss.at[j], h_rs.at[j], ys[j])

    own = ysend[pl.ds(pl.multiple_of(y * SUB, SUB), SUB)]
    proj = mm(own[:, :192], wbuf[0]).astype(BF).astype(F32)
    for j, needed in ((1, (0,)), (3, (1,)), (2, (2, 3))):
        if j == 2:
            for copy in needed:
                wcopies[copy].wait_recv()
        hcopies[j].wait_recv()
        proj = proj + mm(yrecv[j, :, :192], wbuf[j]).astype(BF).astype(F32)
    stream = (resid[...].astype(F32) + rms_scale(proj, attn_gain[...])).astype(BF)
    mixed_ref[...] = stream
    moe_in[...] = rms_scale(stream.astype(F32), ffn_gain[...]).astype(BF)

    z_order = (4, 3, 5, 2, 6, 1, 7)
    x_order = (4, 5, 2, 3, 6, 7, 1)

    def seg(number):
        return pl.ds(pl.multiple_of(number * 8, 8), 8)

    def over_z(src, dst, c, local_sem, ss, rs):
        copies = {
            d: send(
                src.at[c, seg(zs[d])],
                dst.at[c, seg(z)],
                ss.at[c, d],
                rs.at[c, d],
                {"sp_0": zs[d]},
            )
            for d in z_order
        }
        kept = pltpu.make_async_copy(src.at[c, seg(z)], dst.at[c, seg(z)], local_sem.at[c])
        kept.start()
        return copies, kept

    def over_x(src, dst, c, local_sem, ss, rs):
        copies = {}
        for d in x_order:
            a, b = gs[d]
            copies[d] = send(
                src(c, seg(a * NC + b)),
                dst(c, seg(mine)),
                ss.at[c, d],
                rs.at[c, d],
                {"sp_1": a, "sp_2": b},
            )
        kept = pltpu.make_async_copy(src(c, seg(mine)), dst(c, seg(mine)), local_sem.at[c])
        kept.start()
        return copies, kept

    def arrived(moved):
        copies, kept = moved
        kept.wait()
        for copy in copies.values():
            copy.wait_recv()

    def lanes(c):
        h = c % PARTS
        return slice(h * LANES, (h + 1) * LANES)

    z_moves, x_moves, near, far = {}, {}, {}, {}
    sums, joined, back_x, back_z = {}, {}, {}, {}
    high, low = pl.ds(0, HALF), pl.ds(HALF, HALF)

    for s in range(SLOTS):
        place = placing(s).astype(BF)
        for h in range(PARTS):
            c = s * PARTS + h
            sbuf[c] = mm(place, moe_in[:, lanes(c)]).astype(BF)
            z_moves[c] = over_z(sbuf, zbuf, c, zl_sem, z_ss, z_rs)

    def stage_z(c):
        arrived(z_moves[c])
        xsend[c] = mm(order, zbuf[c]).astype(BF)
        x_moves[c] = over_x(
            lambda c, s: xsend.at[c, s], lambda c, s: rows.at[c, 0, s], c, xl_sem, x_ss, x_rs
        )

    def stage_x(c):
        arrived(x_moves[c])
        near[c] = (
            send(rows.at[c, 0], rows.at[c, 1], y_ss.at[c, 0], y_rs.at[c, 0], right),
            send(rows.at[c, 0], rows.at[c, 3], y_ss.at[c, 1], y_rs.at[c, 1], left),
        )

    def stage_near(c):
        near[c][0].wait_recv()
        one = send(rows.at[c, 1, high], rows.at[c, 2, high], y_ss.at[c, 2], y_rs.at[c, 2], right)
        near[c][1].wait_recv()
        two = send(rows.at[c, 3, low], rows.at[c, 2, low], y_ss.at[c, 3], y_rs.at[c, 3], left)
        far[c] = (one, two)

    def stage_gate(c):
        for copy in far[c]:
            copy.wait_recv()
        if c == 0:
            loads[2].wait()
            loads[3].wait()

        def tile(n, carry):
            to = pl.ds(pl.multiple_of(n * HID, 128), HID)
            part = mm(rows[c].reshape(NT * ROWS, LANES), w_in[lanes(c), to])
            if c % PARTS == 0:
                accum[:, to] = part
            else:
                accum[:, to] += part
            return carry

        lax.fori_loop(0, 2, tile, 0)

    def stage_act(s):
        def some(b, carry):
            part = pl.ds(pl.multiple_of(b * 64, 64), 64)
            hidden[part] = (jax.nn.silu(accum[part, :HID]) * accum[part, HID:]).astype(BF)
            return carry

        lax.fori_loop(0, NT * ROWS // 64, some, 0)
        if s == 0:
            loads[4].wait()

    def stage_down(c):
        def tile(n, carry):
            to = pl.ds(pl.multiple_of(n * 256, 256), 256)
            at_lane = pl.ds(pl.multiple_of(c % PARTS * LANES + n * 256, 256), 256)
            part = mm(hidden[...], w_out[:, at_lane]).astype(BF)
            pbuf[c, :, :, to] = part.reshape(NT, ROWS, 256)
            return carry

        lax.fori_loop(0, LANES // 256, tile, 0)
        sums[c] = [
            send(pbuf.at[c, 2, high], relay.at[c, 0], r_ss.at[c, 0], r_rs.at[c, 0], right),
            send(pbuf.at[c, 2, low], relay.at[c, 1], r_ss.at[c, 1], r_rs.at[c, 1], left),
            send(pbuf.at[c, 3, low], ring.at[c, 0, low], r_ss.at[c, 2], r_rs.at[c, 2], right),
            send(pbuf.at[c, 1, high], ring.at[c, 1, high], r_ss.at[c, 3], r_rs.at[c, 3], left),
        ]

    def stage_join(c):
        sums[c][0].wait_recv()
        pbuf[c, 3, :HALF] = (
            pbuf[c, 3, :HALF].astype(F32) + relay[c, 0].astype(F32)
        ).astype(BF)
        one = send(pbuf.at[c, 3, high], ring.at[c, 0, high], r_ss.at[c, 4], r_rs.at[c, 4], right)
        sums[c][1].wait_recv()
        pbuf[c, 1, HALF:] = (
            pbuf[c, 1, HALF:].astype(F32) + relay[c, 1].astype(F32)
        ).astype(BF)
        two = send(pbuf.at[c, 1, low], ring.at[c, 1, low], r_ss.at[c, 5], r_rs.at[c, 5], left)
        joined[c] = (one, two)

    def stage_sum(c):
        for copy in sums[c][2:] + list(joined[c]):
            copy.wait_recv()
        ebuf[c] = (
            pbuf[c, 0].astype(F32) + ring[c, 0].astype(F32) + ring[c, 1].astype(F32)
        ).astype(BF)
        back_x[c] = over_x(
            lambda c, s: ebuf.at[c, s], lambda c, s: xback.at[c, s], c, bl_sem, bx_ss, bx_rs
        )

    def stage_back(c):
        arrived(back_x[c])
        zsend[c] = mm(order_back, xback[c]).astype(BF)
        back_z[c] = over_z(zsend, zback, c, cl_sem, bz_ss, bz_rs)

    def stage_pick(c):
        arrived(back_z[c])
        s = c // PARTS
        part = share[0] * mm(picking(0, s), zback[c]) + share[1] * mm(picking(1, s), zback[c])
        if s == 0:
            branch_ref[:, lanes(c)] = part
        else:
            branch_ref[:, lanes(c)] += part

    stages = {
        "z": stage_z,
        "x": stage_x,
        "near": stage_near,
        "gate": stage_gate,
        "act": stage_act,
        "down": stage_down,
        "join": stage_join,
        "sum": stage_sum,
        "back": stage_back,
        "pick": stage_pick,
    }
    for line in STAGES:
        for word in line.split():
            stages[word[:-1]](int(word[-1]))

    mixed_ref[...] = (
        mixed_ref[...].astype(F32) + rms_scale(branch_ref[...], moe_gain[...])
    ).astype(BF)

    for moves in (z_moves, x_moves, back_x, back_z):
        for copies, _ in moves.values():
            for copy in copies.values():
                copy.wait_send()
    for group in (near, far, sums, joined):
        for copies in group.values():
            for copy in copies:
                copy.wait_send()
    for group in (fwd, bwd, across, qcopies, ocopies, hcopies):
        for copy in group.values():
            copy.wait_send()
    for copy in wcopies:
        copy.wait_send()


def layer(*args):
    dma = pltpu.SemaphoreType.DMA
    vmem = pl.BlockSpec(memory_space=pltpu.VMEM)
    hbm = pl.BlockSpec(memory_space=pl.ANY)
    buf = pltpu.VMEM((CHUNKS, ROWS, LANES), BF)
    return pl.pallas_call(
        layer_kernel,
        out_shape=jax.ShapeDtypeStruct((SUB, D), BF),
        in_specs=[vmem] * 17 + [hbm] * 5,
        out_specs=vmem,
        scratch_shapes=[
            pltpu.VMEM((SUB, D), F32),
            pltpu.VMEM((NX, TOK, 384), BF),
            pltpu.VMEM((NZ, NC, TOK + ROPE, 256), BF),
            pltpu.VMEM((256, 512), BF),
            pltpu.VMEM((6 * TOK, 256), BF),
            pltpu.VMEM((6 * TOK, 128), BF),
            pltpu.VMEM((6 * TOK, 256), BF),
            pltpu.VMEM((6 * TOK, 128), BF),
            pltpu.VMEM((NX, TOK, 128), F32),
            pltpu.VMEM((NX, TOK, 128), F32),
            pltpu.VMEM((NX, TOK, 256), F32),
            pltpu.VMEM((NX, TOK, 128), F32),
            pltpu.VMEM((NX, TOK, 256), BF),
            pltpu.VMEM((NX, TOK, 256), BF),
            pltpu.VMEM((TOK, 256), BF),
            pltpu.VMEM((NT, SUB, 256), BF),
            pltpu.VMEM((NT, 192, D), BF),
            pltpu.VMEM((SUB, D), BF),
            buf,
            buf,
            buf,
            pltpu.VMEM((CHUNKS, NT, ROWS, LANES), BF),
            pltpu.VMEM((D, 2 * HID), BF),
            pltpu.VMEM((HID, D), BF),
            pltpu.VMEM((NT * ROWS, 2 * HID), F32),
            pltpu.VMEM((NT * ROWS, HID), BF),
            pltpu.VMEM((CHUNKS, NT, ROWS, LANES), BF),
            pltpu.VMEM((CHUNKS, 2, HALF, LANES), BF),
            pltpu.VMEM((CHUNKS, 2, ROWS, LANES), BF),
            buf,
            buf,
            buf,
            buf,
            dma((5,)),
            dma((NX,)),
            dma((NX,)),
            dma((5,)),
            dma((5,)),
            dma((5,)),
            dma((5,)),
            dma((9,)),
            dma((9,)),
            dma((NX,)),
            dma((NX,)),
            dma((NT,)),
            dma((NT,)),
            dma((4,)),
            dma((4,)),
            dma((CHUNKS,)),
            dma((CHUNKS, NZ)),
            dma((CHUNKS, NZ)),
            dma((CHUNKS,)),
            dma((CHUNKS, GROUP)),
            dma((CHUNKS, GROUP)),
            dma((CHUNKS, 4)),
            dma((CHUNKS, 4)),
            dma((CHUNKS, 6)),
            dma((CHUNKS, 6)),
            dma((CHUNKS,)),
            dma((CHUNKS, GROUP)),
            dma((CHUNKS, GROUP)),
            dma((CHUNKS,)),
            dma((CHUNKS, NZ)),
            dma((CHUNKS, NZ)),
        ],
        compiler_params=pltpu.CompilerParams(
            collective_id=0, has_side_effects=True, vmem_limit_bytes=58 * 1024 * 1024
        ),
        name="layer",
    )(*args)


def local(
    resid,
    query_wide,
    query_narrow,
    latent,
    rope_key,
    latent_gain,
    key_up_wide,
    value_up_wide,
    key_up_narrow,
    value_up_narrow,
    out_wide,
    out_narrow,
    attn_gain,
    ffn_gain,
    moe_gain,
    routes,
    route_logit,
    expert_gate,
    expert_up,
    expert_down,
):
    positions = lax.axis_index(SP) * TOK + jnp.arange(TOK, dtype=jnp.int32)
    freq = THETA ** (-jnp.arange(ROPE // 2, dtype=jnp.float32) * 2.0 / ROPE)
    angle = freq[:, None] * positions.astype(jnp.float32)[None, :]
    return layer(
        latent,
        latent_gain[None],
        rope_key.T,
        query_wide.T,
        query_narrow,
        jnp.cos(angle),
        jnp.sin(angle),
        key_up_wide,
        value_up_wide,
        key_up_narrow,
        value_up_narrow,
        resid,
        attn_gain[None],
        ffn_gain[None],
        moe_gain[None],
        routes.T,
        route_logit.T,
        out_wide,
        out_narrow,
        expert_gate,
        expert_up,
        expert_down,
    )


def solution(mesh):
    split = Mesh(mesh.devices.reshape(8, 4, 2, mesh.shape["tp"]), ("sp_0", "sp_1", "sp_2", "tp"))
    in_specs = (
        P(SP_TP, None),
        P(SP, "tp"),
        P(SP, "tp"),
        P(SP, None),
        P(SP, None),
        P(),
        P(),
        P(),
        P(),
        P(),
        P("tp", None),
        P("tp", None),
        P(),
        P(),
        P(),
        P(SP_TP, None),
        P(SP_TP, None),
        P(SP, None, "tp"),
        P(SP, None, "tp"),
        P(SP, "tp", None),
    )
    out_specs = P(SP_TP, None)
    return jax.shard_map(local, mesh=split, in_specs=in_specs, out_specs=out_specs, check_vma=False)
```

```python
import functools
import math

import jax
import jax.numpy as jnp
from jax import lax
from jax.experimental import pallas as pl
from jax.experimental.pallas import tpu as pltpu
from jax.sharding import Mesh
from jax.sharding import PartitionSpec as P

NOPE_W = 128
NOPE_N = 64
ROPE = 64
SP = ("sp_0", "sp_1", "sp_2")
SP_TP = ("sp_0", "sp_1", "sp_2", "tp")
NZ, NX, NC, NT = 8, 4, 2, 4
TOK = 256
SUB = 64
D = 2048
LOG2E = math.log2(math.e)
MESH_ID = pl.DeviceIdType.MESH

EPS = 1e-06
THETA = 10000.0

GROUP = NX * NC
SLOTS = 3
WIDE = 1024
PIECES = tuple(
    [(0, n * 512, 512) for n in range(4)]
    + [(1, n * 1024, 1024) for n in range(2)]
    + [(2, n * 512, 512) for n in range(4)]
)
CHUNKS = len(PIECES)
ROWS = NZ * GROUP
HID = 896
HALF = ROWS // 2

FACTOR_W = (NOPE_W + ROPE) ** (-0.5) * LOG2E
FACTOR_N = (NOPE_N + ROPE) ** (-0.5) * LOG2E

BF = jnp.bfloat16
F32 = jnp.float32

SLOT_OF = {0: 0, 1: 1, 7: 2, 2: 3, 6: 4, 3: 5, 5: 6, 4: 7}


def plan(src, dst, send_sem, recv_sem, where):
    return pltpu.make_async_remote_copy(
        src_ref=src,
        dst_ref=dst,
        send_sem=send_sem,
        recv_sem=recv_sem,
        device_id=where,
        device_id_type=MESH_ID,
    )


def send(*args):
    copy = plan(*args)
    copy.start()
    return copy


def mm(a, b):
    return jnp.dot(a, b, preferred_element_type=F32)


def mm_nt(a, b):
    return lax.dot_general(a, b, (((1,), (1,)), ((), ())), preferred_element_type=F32)


def rms_scale(values, gain):
    return values * lax.rsqrt(jnp.mean(values * values, axis=-1, keepdims=True) + EPS) * gain


STAGES = (
    "z0 z1 z2 x0",
    "z3 x1 x2 z4",
    "x3 near0 near1 near2",
    "z5 near3 x4 z8",
    "x5 gate2 gate3 z9",
    "x8 gate0 near4 gate1",
    "z6 z7 act0 near5",
    "down2 down3 x7 down1",
    "x9 near8 gate4 down0",
    "gate5 join3 near9 x6",
    "act1 down4 gate9 join1",
    "gate8 near6 sum3 join4",
    "near7 down5 join2 join0",
    "gate6 sum4 sum1 gate7",
    "join5 act2 down7 back3",
    "sum2 back4 down6 sum0",
    "down9 sum5 back1 back2",
    "join7 back0 join6 down8",
    "back5 join9 sum7 sum6",
    "join8 sum9 pick0 pick3",
    "back7 sum8 pick1 back6",
    "back9 pick4 back8 pick7",
    "pick6 pick2 pick5 pick9",
    "pick8",
)


def layer_kernel(
    latent,
    latent_gain,
    rope_t,
    wide_t,
    narrow_q,
    cosine,
    sine,
    key_wide,
    value_wide,
    key_narrow,
    value_narrow,
    resid,
    attn_gain,
    ffn_gain,
    moe_gain,
    routes_t,
    logit_t,
    out_wide,
    out_narrow,
    gate_hbm,
    up_hbm,
    down_hbm,
    mixed_ref,
    branch_ref,
    nbuf,
    rbuf,
    qbuf,
    kvbuf,
    w_kv,
    kw_s,
    kn_s,
    vw_s,
    vn_s,
    top_w,
    top_n,
    acc_w,
    acc_n,
    osend,
    orecv,
    ysend,
    yrecv,
    wbuf,
    moe_in,
    sbuf,
    zbuf,
    xsend,
    rows,
    w_in,
    w_out,
    accum,
    hidden,
    pbuf,
    relay,
    ring,
    ebuf,
    xback,
    zsend,
    zback,
    l_sem,
    q_ss,
    q_rs,
    f_ss,
    f_rs,
    b_ss,
    b_rs,
    d_ss,
    d_rs,
    o_ss,
    o_rs,
    h_ss,
    h_rs,
    w_ss,
    w_rs,
    zl_sem,
    z_ss,
    z_rs,
    xl_sem,
    x_ss,
    x_rs,
    y_ss,
    y_rs,
    r_ss,
    r_rs,
    bl_sem,
    bx_ss,
    bx_rs,
    cl_sem,
    bz_ss,
    bz_rs,
):
    z = lax.axis_index("sp_0")
    x = lax.axis_index("sp_1")
    core = lax.axis_index("sp_2")
    y = lax.axis_index("tp")
    zs = {d: lax.rem(z + d, NZ) for d in range(1, NZ)}
    gs = {}
    for dx in range(NX):
        for dc in range(NC):
            if dx or dc:
                gs[dx * NC + dc] = (lax.rem(x + dx, NX), lax.rem(core + dc, NC))
    xs = {j: {"sp_1": lax.rem(x + j, NX)} for j in range(1, NX)}
    ys = {j: {"tp": lax.rem(y + j, NT)} for j in range(1, NT)}
    up, down = {"sp_0": zs[1]}, {"sp_0": zs[7]}
    right, left = ys[1], ys[3]
    sibling = {"sp_2": 1 - core}
    mine = x * NC + core

    peers = [{"sp_0": p} for p in zs.values()]
    peers += [{"sp_1": a, "sp_2": b} for a, b in gs.values()]
    peers += list(ys.values())
    barrier = pltpu.get_barrier_semaphore()
    for peer in peers:
        pl.semaphore_signal(barrier, inc=1, device_id=peer, device_id_type=MESH_ID)

    loads = [
        pltpu.make_async_copy(out_wide, wbuf.at[0, pl.ds(0, 128)], l_sem.at[0]),
        pltpu.make_async_copy(out_narrow, wbuf.at[0, pl.ds(128, 64)], l_sem.at[1]),
        pltpu.make_async_copy(gate_hbm.at[0], w_in.at[:, pl.ds(0, HID)], l_sem.at[2]),
        pltpu.make_async_copy(up_hbm.at[0], w_in.at[:, pl.ds(HID, HID)], l_sem.at[3]),
        pltpu.make_async_copy(down_hbm.at[0], w_out, l_sem.at[4]),
    ]
    wide_at = pl.ds(pl.multiple_of(y * 128, 128), 128)
    narrow_at = pl.ds(pl.multiple_of(y // 2 * 128, 128), 128)
    ahead = [
        pltpu.make_async_copy(key_wide.at[:, wide_at], w_kv.at[:, pl.ds(0, 128)], l_sem.at[5]),
        pltpu.make_async_copy(value_wide.at[:, wide_at], w_kv.at[:, pl.ds(256, 128)], l_sem.at[6]),
        pltpu.make_async_copy(key_narrow.at[:, narrow_at], nbuf.at[0], l_sem.at[7]),
        pltpu.make_async_copy(value_narrow.at[:, narrow_at], nbuf.at[1], l_sem.at[8]),
        pltpu.make_async_copy(resid, rbuf, l_sem.at[9]),
    ]
    for load in ahead + loads:
        load.start()

    def turn(values):
        first, second = values[:32].astype(F32), values[32:].astype(F32)
        c, s = cosine[...], sine[...]
        return jnp.concatenate([first * c - second * s, second * c + first * s], axis=0)

    kvbuf[0, 0, :TOK] = rms_scale(latent[...].astype(F32), latent_gain[...]).astype(BF)
    kvbuf[0, 0, TOK:] = turn(rope_t[...]).astype(BF)
    narrow_t = narrow_q[...].astype(F32).T
    qbuf[0, :, :128] = wide_t[:128].astype(F32).T.astype(BF)
    qbuf[0, :, 128:256] = (
        jnp.concatenate([turn(wide_t[128:]), jnp.zeros((64, TOK), F32)], axis=0).T.astype(BF)
    )
    qbuf[0, :, 256:] = (
        jnp.concatenate([narrow_t[:64], turn(narrow_t[64:])], axis=0).T.astype(BF)
    )

    pl.semaphore_wait(barrier, len(peers))

    halves = (pl.ds(0, 160), pl.ds(160, 160))
    first, second = halves
    fwd, bwd, across = {}, {}, {}

    def at(r):
        return SLOT_OF[r % NZ]

    for k in range(1, 5):
        for h, part in enumerate(halves):
            if k < 4 or h == 0:
                fwd[k, h] = plan(
                    kvbuf.at[at(k - 1), 0, part],
                    kvbuf.at[at(k), 0, part],
                    f_ss.at[k, h],
                    f_rs.at[k, h],
                    up,
                )
            if k < 4 or h == 1:
                bwd[k, h] = plan(
                    kvbuf.at[at(1 - k), 0, part],
                    kvbuf.at[at(-k), 0, part],
                    b_ss.at[k, h],
                    b_rs.at[k, h],
                    down,
                )
    for r in (0, 1, 2, 3, 5, 6, 7):
        across[r] = plan(
            kvbuf.at[at(r), 0], kvbuf.at[at(r), 1], d_ss.at[r], d_rs.at[r], sibling
        )
    across[4] = plan(
        kvbuf.at[at(4), 0, first], kvbuf.at[at(4), 1, first], d_ss.at[4], d_rs.at[4], sibling
    )
    across[8] = plan(
        kvbuf.at[at(4), 0, second], kvbuf.at[at(4), 1, second], d_ss.at[8], d_rs.at[8], sibling
    )
    for h in range(2):
        fwd[1, h].start()
        bwd[1, h].start()
    across[0].start()
    qcopies = {
        j: send(qbuf.at[0], qbuf.at[j], q_ss.at[j], q_rs.at[j], xs[j]) for j in (1, 3, 2)
    }
    upper, lower = pl.ds(0, 96), pl.ds(96, 96)
    wcopies = [
        plan(wbuf.at[0], wbuf.at[1], w_ss.at[0], w_rs.at[0], right),
        plan(wbuf.at[0], wbuf.at[3], w_ss.at[1], w_rs.at[1], left),
        plan(wbuf.at[1, upper], wbuf.at[2, upper], w_ss.at[2], w_rs.at[2], right),
        plan(wbuf.at[3, lower], wbuf.at[2, lower], w_ss.at[3], w_rs.at[3], left),
    ]
    loads[0].wait()
    loads[1].wait()
    wcopies[0].start()
    wcopies[1].start()

    lane_w = lax.broadcasted_iota(jnp.int32, (256, 128), 1)
    odd = lax.rem(y, 2) == 1

    def narrow(both):
        return jnp.where(lane_w < 64, jnp.where(odd, pltpu.roll(both, 64, 1), both), 0.0)

    for load in ahead:
        load.wait()
    w_kv[:, 128:256] = narrow(nbuf[0].astype(F32)).astype(BF)
    w_kv[:, 384:] = narrow(nbuf[1].astype(F32)).astype(BF)
    vw_s[:, 128:] = jnp.ones((6 * TOK, 128), BF)

    expert = lax.broadcasted_iota(jnp.int32, (SUB, SUB), 0)
    lane = lax.broadcasted_iota(jnp.int32, (SUB, SUB), 1)
    diagonal = expert == lane

    def column(row):
        return jnp.sum(jnp.where(diagonal, row, 0.0), axis=1, keepdims=True)

    chosen = [routes_t[k : k + 1, :] for k in range(2)]
    named = [(expert == row).astype(F32) for row in chosen]
    earlier = (expert < lane).astype(BF)
    before = mm((named[0] + named[1]).astype(BF), earlier)
    slots = [jnp.sum(before * one, axis=0, keepdims=True) for one in named]
    named_here = [(column(row.astype(F32)) == lane.astype(F32)) for row in chosen]
    slots_here = [column(row) for row in slots]

    def placing(s):
        return jnp.where(slots[0] == s, named[0], 0.0) + jnp.where(slots[1] == s, named[1], 0.0)

    def picking(k, s):
        return jnp.where(named_here[k] & (slots_here[k] == s), 1.0, 0.0).astype(BF)

    logits = [logit_t[k : k + 1, :] for k in range(2)]
    peak = jnp.maximum(logits[0], logits[1])
    parts = [jnp.exp(row - peak) for row in logits]
    share = [column(part / (parts[0] + parts[1])) for part in parts]
    order = (expert // NZ == lax.rem(lane, GROUP)) & (lax.rem(expert, NZ) == lane // GROUP)
    order_back = (expert // GROUP == lax.rem(lane, NZ)) & (lax.rem(expert, GROUP) == lane // NZ)
    order = order.astype(F32).astype(BF)
    order_back = order_back.astype(F32).astype(BF)

    lane_q = lax.broadcasted_iota(jnp.int32, (TOK, 128), 1)

    def expand(base, begin, end):
        def one(i, carry):
            piece = kvbuf[base + i // NC, lax.rem(i, NC)]
            to = pl.ds(pl.multiple_of(i * TOK, TOK), TOK)
            full = mm(piece[:TOK], w_kv[...])
            turned = piece[TOK:].astype(F32)
            tail = jnp.concatenate([turned, turned], axis=0).T
            kw_s[to, :128] = full[:, :128].astype(BF)
            kw_s[to, 128:] = tail.astype(BF)
            kn_s[to] = jnp.where(lane_q < 64, full[:, 128:256], tail).astype(BF)
            vw_s[to, :128] = full[:, 256:384].astype(BF)
            vn_s[to] = jnp.where(lane_q < 64, full[:, 384:], 1.0).astype(BF)
            return carry

        lax.fori_loop(begin, end, one, 0)

    def one_head(q, keys, values, top, acc, j, factor, fresh):
        scores = mm_nt(q, keys)
        best = jnp.max(scores, axis=1, keepdims=True)
        if fresh:
            new = jnp.broadcast_to(best, (TOK, 128))
        else:
            old = top[j]
            new = jnp.maximum(old, best)
            shrink = jnp.exp2((old - new) * factor)
            best = new[:, :1]
        weights = jnp.exp2((scores - best) * factor).astype(BF)
        summed = mm(weights, values)
        if not fresh:
            wide = shrink if summed.shape[1] == 128 else jnp.concatenate([shrink, shrink], axis=1)
            summed = acc[j] * wide + summed
        acc[j] = summed
        top[j] = new

    def attend(j, count, fresh):
        keys = count * NC * TOK
        q = qbuf[j]
        one_head(q[:, :256], kw_s[:keys], vw_s[:keys], top_w, acc_w, j, FACTOR_W, fresh)
        one_head(q[:, 256:], kn_s[:keys], vn_s[:keys], top_n, acc_n, j, FACTOR_N, fresh)

    def forward(k):
        for h in range(2):
            for ring_way in (fwd, bwd):
                ring_way[k, h].wait_recv()
                if (k + 1, h) in ring_way:
                    ring_way[k + 1, h].start()
        across[k].start()
        across[NZ - k].start()

    expand(0, 0, 1)
    across[0].wait_recv()
    expand(0, 1, 2)
    forward(1)
    expand(0, 2, 3)
    across[1].wait_recv()
    expand(0, 3, 5)
    across[7].wait_recv()
    expand(0, 5, 6)

    def first_body(j, carry):
        for other in range(1, NX):

            @pl.when(j == other)
            def _():
                qcopies[other].wait_recv()

        attend(j, 3, True)

        @pl.when(j == 1)
        def _():
            forward(2)

        return carry

    lax.fori_loop(0, NX, first_body, 0)
    for r in (2, 6):
        across[r].wait_recv()
    expand(3, 0, 4)

    def second_body(j, carry):
        attend(j, 2, False)

        @pl.when(j == 0)
        def _():
            forward(3)

        @pl.when(j == 1)
        def _():
            wcopies[0].wait_recv()
            wcopies[2].start()
            wcopies[1].wait_recv()
            wcopies[3].start()

        return carry

    lax.fori_loop(0, NX, second_body, 0)
    for r in (3, 5):
        across[r].wait_recv()
    expand(5, 0, 4)
    fwd[4, 0].wait_recv()
    across[4].start()
    bwd[4, 1].wait_recv()
    across[8].start()
    for r in (4, 8):
        across[r].wait_recv()
    expand(5, 4, 6)

    def three(value):
        high = value.astype(BF).astype(F32)
        rest = value - high
        middle = rest.astype(BF).astype(F32)
        return high, middle, rest - middle

    def finish(j):
        total_w = acc_w[j, :, 128:]
        osend[j, :, :128] = (acc_w[j, :, :128] / total_w).astype(BF)
        both = acc_n[j]
        tail = both / pltpu.roll(both, 64, 1)
        level_w = top_w[j] * FACTOR_W + jnp.log2(total_w)
        level_n = top_n[j] * FACTOR_N + jnp.log2(both)
        at_lane = 64
        for part in three(level_w) + three(level_n):
            tail = jnp.where(lane_q == at_lane, part, tail)
            at_lane += 1
        osend[j, :, 128:] = tail.astype(BF)

    ocopies = {
        j: plan(osend.at[j], orecv.at[j], o_ss.at[j], o_rs.at[j], xs[NX - j]) for j in (1, 2, 3)
    }

    def last_body(i, carry):
        j = 2 + i - i // 2 * (2 * i - 1)
        attend(j, 3, False)
        finish(j)
        for other in range(1, NX):

            @pl.when(j == other)
            def _():
                ocopies[other].start()

        return carry

    lax.fori_loop(0, NX, last_body, 0)
    for j in (2, 3, 1):
        ocopies[j].wait_recv()

    tails = [osend[0, :, 128:].astype(F32)] + [orecv[j, :, 128:].astype(F32) for j in (1, 2, 3)]
    mains = [osend[0, :, :128]] + [orecv[j, :, :128] for j in (1, 2, 3)]

    def weigh(a):
        levels = [(t[:, a : a + 1] + t[:, a + 1 : a + 2]) + t[:, a + 2 : a + 3] for t in tails]
        best = functools.reduce(jnp.maximum, levels)
        portions = [jnp.exp2(level - best) for level in levels]
        total = functools.reduce(jnp.add, portions)
        return [portion / total for portion in portions]

    merged_w = functools.reduce(jnp.add, [m.astype(F32) * s for m, s in zip(mains, weigh(64))])
    merged_n = functools.reduce(jnp.add, [t * s for t, s in zip(tails, weigh(67))])
    ysend[:, :128] = merged_w.astype(BF)
    ysend[:, 128:] = jnp.where(lane_q < 64, merged_n, 0.0).astype(BF)
    hcopies = {}
    for j in (2, 1, 3):
        part = pl.ds(pl.multiple_of(lax.rem(y + j, NT) * SUB, SUB), SUB)
        hcopies[j] = send(ysend.at[part], yrecv.at[j], h_ss.at[j], h_rs.at[j], ys[j])

    own = ysend[pl.ds(pl.multiple_of(y * SUB, SUB), SUB)]
    proj = mm(own[:, :192], wbuf[0]).astype(BF).astype(F32)
    for j, needed in ((1, (0,)), (3, (1,)), (2, (2, 3))):
        if j == 2:
            for copy in needed:
                wcopies[copy].wait_recv()
        hcopies[j].wait_recv()
        proj = proj + mm(yrecv[j, :, :192], wbuf[j]).astype(BF).astype(F32)
    stream = (rbuf[...].astype(F32) + rms_scale(proj, attn_gain[...])).astype(BF)
    mixed_ref[...] = stream
    moe_in[...] = rms_scale(stream.astype(F32), ffn_gain[...]).astype(BF)

    z_order = (4, 3, 5, 2, 6, 1, 7)
    x_order = (4, 5, 2, 3, 6, 7, 1)

    def seg(number):
        return pl.ds(pl.multiple_of(number * 8, 8), 8)

    def across_lanes(c):
        return pl.ds(0, PIECES[c][2])

    def over_z(src, dst, c, local_sem, ss, rs):
        copies = {
            d: send(
                src.at[c, seg(zs[d]), across_lanes(c)],
                dst.at[c, seg(z), across_lanes(c)],
                ss.at[c, d],
                rs.at[c, d],
                {"sp_0": zs[d]},
            )
            for d in z_order
        }
        kept = pltpu.make_async_copy(
            src.at[c, seg(z), across_lanes(c)], dst.at[c, seg(z), across_lanes(c)], local_sem.at[c]
        )
        kept.start()
        return copies, kept

    def over_x(src, dst, c, local_sem, ss, rs):
        copies = {}
        for d in x_order:
            a, b = gs[d]
            copies[d] = send(
                src(c, seg(a * NC + b)),
                dst(c, seg(mine)),
                ss.at[c, d],
                rs.at[c, d],
                {"sp_1": a, "sp_2": b},
            )
        kept = pltpu.make_async_copy(src(c, seg(mine)), dst(c, seg(mine)), local_sem.at[c])
        kept.start()
        return copies, kept

    def arrived(moved):
        copies, kept = moved
        kept.wait()
        for copy in copies.values():
            copy.wait_recv()

    def lanes(c):
        return slice(PIECES[c][1], PIECES[c][1] + PIECES[c][2])

    def here(c):
        return slice(0, PIECES[c][2])

    z_moves, x_moves, near, far = {}, {}, {}, {}
    sums, joined, back_x, back_z = {}, {}, {}, {}
    high, low, whole = pl.ds(0, HALF), pl.ds(HALF, HALF), pl.ds(0, ROWS)
    begun = set()

    def hop(src, src_at, dst, dst_at, part, ss, rs, n, where):
        c = src_at[0]
        return send(
            src.at[(*src_at, part, across_lanes(c))],
            dst.at[(*dst_at, part, across_lanes(c))],
            ss.at[c, n],
            rs.at[c, n],
            where,
        )

    branch_ref[...] = jnp.zeros((SUB, D), F32)
    for c in range(CHUNKS):
        place = placing(PIECES[c][0]).astype(BF)
        sbuf[c, :, here(c)] = mm(place, moe_in[:, lanes(c)]).astype(BF)
        z_moves[c] = over_z(sbuf, zbuf, c, zl_sem, z_ss, z_rs)

    def stage_z(c):
        arrived(z_moves[c])
        xsend[c, :, here(c)] = mm(order, zbuf[c, :, here(c)]).astype(BF)
        x_moves[c] = over_x(
            lambda c, s: xsend.at[c, s, across_lanes(c)],
            lambda c, s: rows.at[c, 0, s, across_lanes(c)],
            c,
            xl_sem,
            x_ss,
            x_rs,
        )

    def stage_x(c):
        arrived(x_moves[c])
        near[c] = (
            hop(rows, (c, 0), rows, (c, 1), whole, y_ss, y_rs, 0, right),
            hop(rows, (c, 0), rows, (c, 3), whole, y_ss, y_rs, 1, left),
        )

    def stage_near(c):
        near[c][0].wait_recv()
        one = hop(rows, (c, 1), rows, (c, 2), high, y_ss, y_rs, 2, right)
        near[c][1].wait_recv()
        two = hop(rows, (c, 3), rows, (c, 2), low, y_ss, y_rs, 3, left)
        far[c] = (one, two)

    def stage_gate(c):
        for copy in far[c]:
            copy.wait_recv()
        if not begun:
            loads[2].wait()
            loads[3].wait()
        slot = PIECES[c][0]
        fresh = slot not in begun
        begun.add(slot)

        def tile(n, carry):
            to = pl.ds(pl.multiple_of(n * HID, 128), HID)
            held = rows[c, :, :, here(c)].reshape(NT * ROWS, PIECES[c][2])
            part = mm(held, w_in[lanes(c), to])
            if fresh:
                accum[:, to] = part
            else:
                accum[:, to] += part
            return carry

        lax.fori_loop(0, 2, tile, 0)

    def stage_act(s):
        def some(b, carry):
            part = pl.ds(pl.multiple_of(b * 64, 64), 64)
            hidden[part] = (jax.nn.silu(accum[part, :HID]) * accum[part, HID:]).astype(BF)
            return carry

        lax.fori_loop(0, NT * ROWS // 64, some, 0)
        if s == 0:
            loads[4].wait()

    def stage_down(c):
        def tile(n, carry):
            to = pl.ds(pl.multiple_of(n * 256, 256), 256)
            at_lane = pl.ds(pl.multiple_of(PIECES[c][1] + n * 256, 256), 256)
            part = mm(hidden[...], w_out[:, at_lane]).astype(BF)
            pbuf[c, :, :, to] = part.reshape(NT, ROWS, 256)
            return carry

        lax.fori_loop(0, PIECES[c][2] // 256, tile, 0)
        sums[c] = [
            hop(pbuf, (c, 2), relay, (c, 0), high, r_ss, r_rs, 0, right),
            hop(pbuf, (c, 2), relay, (c, 0), low, r_ss, r_rs, 1, left),
            hop(pbuf, (c, 3), ring, (c, 0), low, r_ss, r_rs, 2, right),
            hop(pbuf, (c, 1), ring, (c, 1), high, r_ss, r_rs, 3, left),
        ]

    def stage_join(c):
        at_lanes = here(c)
        sums[c][0].wait_recv()
        pbuf[c, 3, :HALF, at_lanes] = (
            pbuf[c, 3, :HALF, at_lanes].astype(F32) + relay[c, 0, :HALF, at_lanes].astype(F32)
        ).astype(BF)
        one = hop(pbuf, (c, 3), ring, (c, 0), high, r_ss, r_rs, 4, right)
        sums[c][1].wait_recv()
        pbuf[c, 1, HALF:, at_lanes] = (
            pbuf[c, 1, HALF:, at_lanes].astype(F32) + relay[c, 0, HALF:, at_lanes].astype(F32)
        ).astype(BF)
        two = hop(pbuf, (c, 1), ring, (c, 1), low, r_ss, r_rs, 5, left)
        joined[c] = (one, two)

    def stage_sum(c):
        for copy in sums[c][2:] + list(joined[c]):
            copy.wait_recv()
        ebuf[c, :, here(c)] = (
            pbuf[c, 0, :, here(c)].astype(F32)
            + ring[c, 0, :, here(c)].astype(F32)
            + ring[c, 1, :, here(c)].astype(F32)
        ).astype(BF)
        back_x[c] = over_x(
            lambda c, s: ebuf.at[c, s, across_lanes(c)],
            lambda c, s: xback.at[c, s, across_lanes(c)],
            c,
            bl_sem,
            bx_ss,
            bx_rs,
        )

    def stage_back(c):
        arrived(back_x[c])
        zsend[c, :, here(c)] = mm(order_back, xback[c, :, here(c)]).astype(BF)
        back_z[c] = over_z(zsend, zback, c, cl_sem, bz_ss, bz_rs)

    def stage_pick(c):
        arrived(back_z[c])
        s = PIECES[c][0]
        back = zback[c, :, here(c)]
        branch_ref[:, lanes(c)] += share[0] * mm(picking(0, s), back) + share[1] * mm(
            picking(1, s), back
        )

    stages = {
        "z": stage_z,
        "x": stage_x,
        "near": stage_near,
        "gate": stage_gate,
        "act": stage_act,
        "down": stage_down,
        "join": stage_join,
        "sum": stage_sum,
        "back": stage_back,
        "pick": stage_pick,
    }
    for line in STAGES:
        for word in line.split():
            stages[word[:-1]](int(word[-1]))

    mixed_ref[...] = (
        mixed_ref[...].astype(F32) + rms_scale(branch_ref[...], moe_gain[...])
    ).astype(BF)

    for moves in (z_moves, x_moves, back_x, back_z):
        for copies, _ in moves.values():
            for copy in copies.values():
                copy.wait_send()
    for group in (near, far, sums, joined):
        for copies in group.values():
            for copy in copies:
                copy.wait_send()
    for group in (fwd, bwd, across, qcopies, ocopies, hcopies):
        for copy in group.values():
            copy.wait_send()
    for copy in wcopies:
        copy.wait_send()


def layer(*args):
    dma = pltpu.SemaphoreType.DMA
    vmem = pl.BlockSpec(memory_space=pltpu.VMEM)
    hbm = pl.BlockSpec(memory_space=pl.ANY)
    buf = pltpu.VMEM((CHUNKS, ROWS, WIDE), BF)
    return pl.pallas_call(
        layer_kernel,
        out_shape=jax.ShapeDtypeStruct((SUB, D), BF),
        in_specs=[vmem] * 7 + [hbm] * 5 + [vmem] * 5 + [hbm] * 5,
        out_specs=vmem,
        scratch_shapes=[
            pltpu.VMEM((SUB, D), F32),
            pltpu.VMEM((2, 256, 128), BF),
            pltpu.VMEM((SUB, D), BF),
            pltpu.VMEM((NX, TOK, 384), BF),
            pltpu.VMEM((NZ, NC, TOK + ROPE, 256), BF),
            pltpu.VMEM((256, 512), BF),
            pltpu.VMEM((6 * TOK, 256), BF),
            pltpu.VMEM((6 * TOK, 128), BF),
            pltpu.VMEM((6 * TOK, 256), BF),
            pltpu.VMEM((6 * TOK, 128), BF),
            pltpu.VMEM((NX, TOK, 128), F32),
            pltpu.VMEM((NX, TOK, 128), F32),
            pltpu.VMEM((NX, TOK, 256), F32),
            pltpu.VMEM((NX, TOK, 128), F32),
            pltpu.VMEM((NX, TOK, 256), BF),
            pltpu.VMEM((NX, TOK, 256), BF),
            pltpu.VMEM((TOK, 256), BF),
            pltpu.VMEM((NT, SUB, 256), BF),
            pltpu.VMEM((NT, 192, D), BF),
            pltpu.VMEM((SUB, D), BF),
            buf,
            buf,
            buf,
            pltpu.VMEM((CHUNKS, NT, ROWS, WIDE), BF),
            pltpu.VMEM((D, 2 * HID), BF),
            pltpu.VMEM((HID, D), BF),
            pltpu.VMEM((NT * ROWS, 2 * HID), F32),
            pltpu.VMEM((NT * ROWS, HID), BF),
            pltpu.VMEM((CHUNKS, NT, ROWS, WIDE), BF),
            pltpu.VMEM((CHUNKS, 1, ROWS, WIDE), BF),
            pltpu.VMEM((CHUNKS, 2, ROWS, WIDE), BF),
            buf,
            buf,
            buf,
            buf,
            dma((10,)),
            dma((NX,)),
            dma((NX,)),
            dma((5, 2)),
            dma((5, 2)),
            dma((5, 2)),
            dma((5, 2)),
            dma((9,)),
            dma((9,)),
            dma((NX,)),
            dma((NX,)),
            dma((NT,)),
            dma((NT,)),
            dma((4,)),
            dma((4,)),
            dma((CHUNKS,)),
            dma((CHUNKS, NZ)),
            dma((CHUNKS, NZ)),
            dma((CHUNKS,)),
            dma((CHUNKS, GROUP)),
            dma((CHUNKS, GROUP)),
            dma((CHUNKS, 4)),
            dma((CHUNKS, 4)),
            dma((CHUNKS, 6)),
            dma((CHUNKS, 6)),
            dma((CHUNKS,)),
            dma((CHUNKS, GROUP)),
            dma((CHUNKS, GROUP)),
            dma((CHUNKS,)),
            dma((CHUNKS, NZ)),
            dma((CHUNKS, NZ)),
        ],
        compiler_params=pltpu.CompilerParams(
            collective_id=0, has_side_effects=True, vmem_limit_bytes=58 * 1024 * 1024
        ),
        name="layer",
    )(*args)


def local(
    resid,
    query_wide,
    query_narrow,
    latent,
    rope_key,
    latent_gain,
    key_up_wide,
    value_up_wide,
    key_up_narrow,
    value_up_narrow,
    out_wide,
    out_narrow,
    attn_gain,
    ffn_gain,
    moe_gain,
    routes,
    route_logit,
    expert_gate,
    expert_up,
    expert_down,
):
    positions = lax.axis_index(SP) * TOK + jnp.arange(TOK, dtype=jnp.int32)
    freq = THETA ** (-jnp.arange(ROPE // 2, dtype=jnp.float32) * 2.0 / ROPE)
    angle = freq[:, None] * positions.astype(jnp.float32)[None, :]
    return layer(
        latent,
        latent_gain[None],
        rope_key.T,
        query_wide.T,
        query_narrow,
        jnp.cos(angle),
        jnp.sin(angle),
        key_up_wide,
        value_up_wide,
        key_up_narrow,
        value_up_narrow,
        resid,
        attn_gain[None],
        ffn_gain[None],
        moe_gain[None],
        routes.T,
        route_logit.T,
        out_wide,
        out_narrow,
        expert_gate,
        expert_up,
        expert_down,
    )


def solution(mesh):
    split = Mesh(mesh.devices.reshape(8, 4, 2, mesh.shape["tp"]), ("sp_0", "sp_1", "sp_2", "tp"))
    in_specs = (
        P(SP_TP, None),
        P(SP, "tp"),
        P(SP, "tp"),
        P(SP, None),
        P(SP, None),
        P(),
        P(),
        P(),
        P(),
        P(),
        P("tp", None),
        P("tp", None),
        P(),
        P(),
        P(),
        P(SP_TP, None),
        P(SP_TP, None),
        P(SP, None, "tp"),
        P(SP, None, "tp"),
        P(SP, "tp", None),
    )
    out_specs = P(SP_TP, None)
    return jax.shard_map(local, mesh=split, in_specs=in_specs, out_specs=out_specs, check_vma=False)
```

```python
import functools
import math

import jax
import jax.numpy as jnp
from jax import lax
from jax.experimental import pallas as pl
from jax.experimental.pallas import tpu as pltpu
from jax.sharding import Mesh
from jax.sharding import PartitionSpec as P

NOPE_W = 128
NOPE_N = 64
ROPE = 64
SP = ("sp_0", "sp_1", "sp_2")
SP_TP = ("sp_0", "sp_1", "sp_2", "tp")
NZ, NX, NC, NT = 8, 4, 2, 4
TOK = 256
SUB = 64
D = 2048
LOG2E = math.log2(math.e)
MESH_ID = pl.DeviceIdType.MESH

EPS = 1e-06
THETA = 10000.0

GROUP = NX * NC
SLOTS = 3
WIDE = 1024
PIECES = tuple(
    [(0, n * 512, 512) for n in range(4)]
    + [(1, n * 1024, 1024) for n in range(2)]
    + [(2, n * 512, 512) for n in range(4)]
)
CHUNKS = len(PIECES)
ROWS = NZ * GROUP
HID = 896
HALF = ROWS // 2

FACTOR_W = (NOPE_W + ROPE) ** (-0.5) * LOG2E
FACTOR_N = (NOPE_N + ROPE) ** (-0.5) * LOG2E

BF = jnp.bfloat16
F32 = jnp.float32

SLOT_OF = {0: 0, 1: 1, 7: 2, 2: 3, 6: 4, 3: 5, 5: 6, 4: 7}


def plan(src, dst, send_sem, recv_sem, where):
    return pltpu.make_async_remote_copy(
        src_ref=src,
        dst_ref=dst,
        send_sem=send_sem,
        recv_sem=recv_sem,
        device_id=where,
        device_id_type=MESH_ID,
    )


def send(*args):
    copy = plan(*args)
    copy.start()
    return copy


def mm(a, b):
    return jnp.dot(a, b, preferred_element_type=F32)


def mm_nt(a, b):
    return lax.dot_general(a, b, (((1,), (1,)), ((), ())), preferred_element_type=F32)


def rms_scale(values, gain):
    return values * lax.rsqrt(jnp.mean(values * values, axis=-1, keepdims=True) + EPS) * gain


STAGES = (
    "z0 z1 z2 x0",
    "z3 x1 x2 z4",
    "x3 near0 near1 near2",
    "z5 near3 x4 z8",
    "x5 gate2 gate3 z9",
    "x8 gate0 near4 gate1",
    "z6 z7 act0 near5",
    "down2 down3 x7 down1",
    "x9 near8 gate4 down0",
    "gate5 join3 near9 x6",
    "act1 down4 gate9 join1",
    "gate8 near6 sum3 join4",
    "near7 down5 join2 join0",
    "gate6 sum4 sum1 gate7",
    "join5 act2 down7 back3",
    "sum2 back4 down6 sum0",
    "down9 sum5 back1 back2",
    "join7 back0 join6 down8",
    "back5 join9 sum7 sum6",
    "join8 sum9 pick0 pick3",
    "back7 sum8 pick1 back6",
    "back9 pick4 back8 pick7",
    "pick6 pick2 pick5 pick9",
    "pick8",
)


def layer_kernel(
    latent,
    latent_gain,
    rope_t,
    wide_t,
    narrow_q,
    cosine,
    sine,
    key_wide,
    value_wide,
    key_narrow,
    value_narrow,
    resid,
    attn_gain,
    ffn_gain,
    moe_gain,
    routes_t,
    logit_t,
    out_wide,
    out_narrow,
    gate_hbm,
    up_hbm,
    down_hbm,
    mixed_ref,
    branch_ref,
    nbuf,
    rbuf,
    qbuf,
    kvbuf,
    w_kv,
    kw_s,
    kn_s,
    vw_s,
    vn_s,
    top_w,
    top_n,
    acc_w,
    acc_n,
    osend,
    orecv,
    ysend,
    yrecv,
    wbuf,
    moe_in,
    sbuf,
    zbuf,
    xsend,
    rows,
    w_in,
    w_out,
    accum,
    hidden,
    pbuf,
    relay,
    ring,
    ebuf,
    xback,
    zsend,
    zback,
    l_sem,
    q_ss,
    q_rs,
    f_ss,
    f_rs,
    b_ss,
    b_rs,
    d_ss,
    d_rs,
    o_ss,
    o_rs,
    h_ss,
    h_rs,
    w_ss,
    w_rs,
    zl_sem,
    z_ss,
    z_rs,
    xl_sem,
    x_ss,
    x_rs,
    y_ss,
    y_rs,
    r_ss,
    r_rs,
    bl_sem,
    bx_ss,
    bx_rs,
    cl_sem,
    bz_ss,
    bz_rs,
):
    z = lax.axis_index("sp_0")
    x = lax.axis_index("sp_1")
    core = lax.axis_index("sp_2")
    y = lax.axis_index("tp")
    zs = {d: lax.rem(z + d, NZ) for d in range(1, NZ)}
    gs = {}
    for dx in range(NX):
        for dc in range(NC):
            if dx or dc:
                gs[dx * NC + dc] = (lax.rem(x + dx, NX), lax.rem(core + dc, NC))
    xs = {j: {"sp_1": lax.rem(x + j, NX)} for j in range(1, NX)}
    ys = {j: {"tp": lax.rem(y + j, NT)} for j in range(1, NT)}
    up, down = {"sp_0": zs[1]}, {"sp_0": zs[7]}
    right, left = ys[1], ys[3]
    sibling = {"sp_2": 1 - core}
    mine = x * NC + core

    peers = [{"sp_0": p} for p in zs.values()]
    peers += [{"sp_1": a, "sp_2": b} for a, b in gs.values()]
    peers += list(ys.values())
    barrier = pltpu.get_barrier_semaphore()
    for peer in peers:
        pl.semaphore_signal(barrier, inc=1, device_id=peer, device_id_type=MESH_ID)

    loads = [
        pltpu.make_async_copy(out_wide, wbuf.at[0, pl.ds(0, 128)], l_sem.at[0]),
        pltpu.make_async_copy(out_narrow, wbuf.at[0, pl.ds(128, 64)], l_sem.at[1]),
        pltpu.make_async_copy(gate_hbm.at[0], w_in.at[:, pl.ds(0, HID)], l_sem.at[2]),
        pltpu.make_async_copy(up_hbm.at[0], w_in.at[:, pl.ds(HID, HID)], l_sem.at[3]),
        pltpu.make_async_copy(down_hbm.at[0], w_out, l_sem.at[4]),
    ]
    wide_at = pl.ds(pl.multiple_of(y * 128, 128), 128)
    narrow_at = pl.ds(pl.multiple_of(y // 2 * 128, 128), 128)
    ahead = [
        pltpu.make_async_copy(key_wide.at[:, wide_at], w_kv.at[:, pl.ds(0, 128)], l_sem.at[5]),
        pltpu.make_async_copy(value_wide.at[:, wide_at], w_kv.at[:, pl.ds(256, 128)], l_sem.at[6]),
        pltpu.make_async_copy(key_narrow.at[:, narrow_at], nbuf.at[0], l_sem.at[7]),
        pltpu.make_async_copy(value_narrow.at[:, narrow_at], nbuf.at[1], l_sem.at[8]),
        pltpu.make_async_copy(resid, rbuf, l_sem.at[9]),
    ]
    for load in ahead + loads:
        load.start()

    def turn(values):
        first, second = values[:32].astype(F32), values[32:].astype(F32)
        c, s = cosine[...], sine[...]
        return jnp.concatenate([first * c - second * s, second * c + first * s], axis=0)

    kvbuf[0, 0, :TOK] = rms_scale(latent[...].astype(F32), latent_gain[...]).astype(BF)
    kvbuf[0, 0, TOK:] = turn(rope_t[...]).astype(BF)
    narrow_t = narrow_q[...].astype(F32).T
    qbuf[0, :, :128] = wide_t[:128].astype(F32).T.astype(BF)
    qbuf[0, :, 128:256] = (
        jnp.concatenate([turn(wide_t[128:]), jnp.zeros((64, TOK), F32)], axis=0).T.astype(BF)
    )
    qbuf[0, :, 256:] = (
        jnp.concatenate([narrow_t[:64], turn(narrow_t[64:])], axis=0).T.astype(BF)
    )

    pl.semaphore_wait(barrier, len(peers))

    halves = (pl.ds(0, 160), pl.ds(160, 160))
    first, second = halves
    fwd, bwd, across = {}, {}, {}

    def at(r):
        return SLOT_OF[r % NZ]

    for k in range(1, 5):
        for h, part in enumerate(halves):
            if k < 4 or h == 0:
                fwd[k, h] = plan(
                    kvbuf.at[at(k - 1), 0, part],
                    kvbuf.at[at(k), 0, part],
                    f_ss.at[k, h],
                    f_rs.at[k, h],
                    up,
                )
            if k < 4 or h == 1:
                bwd[k, h] = plan(
                    kvbuf.at[at(1 - k), 0, part],
                    kvbuf.at[at(-k), 0, part],
                    b_ss.at[k, h],
                    b_rs.at[k, h],
                    down,
                )
    for r in (0, 1, 2, 3, 5, 6, 7):
        across[r] = plan(
            kvbuf.at[at(r), 0], kvbuf.at[at(r), 1], d_ss.at[r], d_rs.at[r], sibling
        )
    across[4] = plan(
        kvbuf.at[at(4), 0, first], kvbuf.at[at(4), 1, first], d_ss.at[4], d_rs.at[4], sibling
    )
    across[8] = plan(
        kvbuf.at[at(4), 0, second], kvbuf.at[at(4), 1, second], d_ss.at[8], d_rs.at[8], sibling
    )
    for h in range(2):
        fwd[1, h].start()
        bwd[1, h].start()
    across[0].start()
    qcopies = {
        j: send(qbuf.at[0], qbuf.at[j], q_ss.at[j], q_rs.at[j], xs[j]) for j in (1, 3, 2)
    }
    upper, lower = pl.ds(0, 96), pl.ds(96, 96)
    wcopies = [
        plan(wbuf.at[0], wbuf.at[1], w_ss.at[0], w_rs.at[0], right),
        plan(wbuf.at[0], wbuf.at[3], w_ss.at[1], w_rs.at[1], left),
        plan(wbuf.at[1, upper], wbuf.at[2, upper], w_ss.at[2], w_rs.at[2], right),
        plan(wbuf.at[3, lower], wbuf.at[2, lower], w_ss.at[3], w_rs.at[3], left),
    ]
    loads[0].wait()
    loads[1].wait()
    wcopies[0].start()
    wcopies[1].start()

    lane_w = lax.broadcasted_iota(jnp.int32, (256, 128), 1)
    odd = lax.rem(y, 2) == 1

    def narrow(both):
        return jnp.where(lane_w < 64, jnp.where(odd, pltpu.roll(both, 64, 1), both), 0.0)

    for load in ahead:
        load.wait()
    w_kv[:, 128:256] = narrow(nbuf[0].astype(F32)).astype(BF)
    w_kv[:, 384:] = narrow(nbuf[1].astype(F32)).astype(BF)
    vw_s[:, 128:] = jnp.ones((6 * TOK, 128), BF)

    expert = lax.broadcasted_iota(jnp.int32, (SUB, SUB), 0)
    lane = lax.broadcasted_iota(jnp.int32, (SUB, SUB), 1)
    diagonal = expert == lane

    def column(row):
        return jnp.sum(jnp.where(diagonal, row, 0.0), axis=1, keepdims=True)

    chosen = [routes_t[k : k + 1, :] for k in range(2)]
    named = [(expert == row).astype(F32) for row in chosen]
    earlier = (expert < lane).astype(BF)
    before = mm((named[0] + named[1]).astype(BF), earlier)
    slots = [jnp.sum(before * one, axis=0, keepdims=True) for one in named]
    named_here = [(column(row.astype(F32)) == lane.astype(F32)) for row in chosen]
    slots_here = [column(row) for row in slots]

    def placing(s):
        return jnp.where(slots[0] == s, named[0], 0.0) + jnp.where(slots[1] == s, named[1], 0.0)

    def picking(k, s):
        return jnp.where(named_here[k] & (slots_here[k] == s), 1.0, 0.0).astype(BF)

    logits = [logit_t[k : k + 1, :] for k in range(2)]
    peak = jnp.maximum(logits[0], logits[1])
    parts = [jnp.exp(row - peak) for row in logits]
    share = [column(part / (parts[0] + parts[1])) for part in parts]
    order = (expert // NZ == lax.rem(lane, GROUP)) & (lax.rem(expert, NZ) == lane // GROUP)
    order_back = (expert // GROUP == lax.rem(lane, NZ)) & (lax.rem(expert, GROUP) == lane // NZ)
    order = order.astype(F32).astype(BF)
    order_back = order_back.astype(F32).astype(BF)

    lane_q = lax.broadcasted_iota(jnp.int32, (TOK, 128), 1)

    def expand(base, begin, end):
        def one(i, carry):
            piece = kvbuf[base + i // NC, lax.rem(i, NC)]
            to = pl.ds(pl.multiple_of(i * TOK, TOK), TOK)
            full = mm(piece[:TOK], w_kv[...])
            turned = piece[TOK:].astype(F32)
            tail = jnp.concatenate([turned, turned], axis=0).T
            kw_s[to, :128] = full[:, :128].astype(BF)
            kw_s[to, 128:] = tail.astype(BF)
            kn_s[to] = jnp.where(lane_q < 64, full[:, 128:256], tail).astype(BF)
            vw_s[to, :128] = full[:, 256:384].astype(BF)
            vn_s[to] = jnp.where(lane_q < 64, full[:, 384:], 1.0).astype(BF)
            return carry

        lax.fori_loop(begin, end, one, 0)

    def one_head(q, keys, values, top, acc, j, factor, fresh):
        scores = mm_nt(q, keys)
        best = jnp.max(scores, axis=1, keepdims=True)
        if fresh:
            new = jnp.broadcast_to(best, (TOK, 128))
        else:
            old = top[j]
            new = jnp.maximum(old, best)
            shrink = jnp.exp2((old - new) * factor)
            best = new[:, :1]
        weights = jnp.exp2((scores - best) * factor).astype(BF)
        summed = mm(weights, values)
        if not fresh:
            wide = shrink if summed.shape[1] == 128 else jnp.concatenate([shrink, shrink], axis=1)
            summed = acc[j] * wide + summed
        acc[j] = summed
        top[j] = new

    def attend(j, count, fresh):
        keys = count * NC * TOK
        q = qbuf[j]
        one_head(q[:, :256], kw_s[:keys], vw_s[:keys], top_w, acc_w, j, FACTOR_W, fresh)
        one_head(q[:, 256:], kn_s[:keys], vn_s[:keys], top_n, acc_n, j, FACTOR_N, fresh)

    def forward(k):
        for h in range(2):
            for ring_way in (fwd, bwd):
                ring_way[k, h].wait_recv()
                if (k + 1, h) in ring_way:
                    ring_way[k + 1, h].start()
        across[k].start()
        across[NZ - k].start()

    expand(0, 0, 1)
    across[0].wait_recv()
    expand(0, 1, 2)
    forward(1)
    expand(0, 2, 3)
    across[1].wait_recv()
    expand(0, 3, 5)
    across[7].wait_recv()
    expand(0, 5, 6)

    def first_body(j, carry):
        for other in range(1, NX):

            @pl.when(j == other)
            def _():
                qcopies[other].wait_recv()

        attend(j, 3, True)

        @pl.when(j == 1)
        def _():
            forward(2)

        return carry

    lax.fori_loop(0, NX, first_body, 0)
    for r in (2, 6):
        across[r].wait_recv()
    expand(3, 0, 4)

    def second_body(j, carry):
        attend(j, 2, False)

        @pl.when(j == 0)
        def _():
            forward(3)

        return carry

    lax.fori_loop(0, NX, second_body, 0)
    for r in (3, 5):
        across[r].wait_recv()
    expand(5, 0, 4)
    fwd[4, 0].wait_recv()
    across[4].start()
    bwd[4, 1].wait_recv()
    across[8].start()
    for r in (4, 8):
        across[r].wait_recv()
    expand(5, 4, 6)

    def three(value):
        high = value.astype(BF).astype(F32)
        rest = value - high
        middle = rest.astype(BF).astype(F32)
        return high, middle, rest - middle

    def finish(j):
        total_w = acc_w[j, :, 128:]
        osend[j, :, :128] = (acc_w[j, :, :128] / total_w).astype(BF)
        both = acc_n[j]
        tail = both / pltpu.roll(both, 64, 1)
        level_w = top_w[j] * FACTOR_W + jnp.log2(total_w)
        level_n = top_n[j] * FACTOR_N + jnp.log2(both)
        at_lane = 64
        for part in three(level_w) + three(level_n):
            tail = jnp.where(lane_q == at_lane, part, tail)
            at_lane += 1
        osend[j, :, 128:] = tail.astype(BF)

    ocopies = {
        j: plan(osend.at[j], orecv.at[j], o_ss.at[j], o_rs.at[j], xs[NX - j]) for j in (1, 2, 3)
    }

    def last_body(i, carry):
        j = 2 + i - i // 2 * (2 * i - 1)
        @pl.when(i == 1)
        def _():
            wcopies[0].wait_recv()
            wcopies[2].start()
            wcopies[1].wait_recv()
            wcopies[3].start()

        attend(j, 3, False)
        finish(j)
        for other in range(1, NX):

            @pl.when(j == other)
            def _():
                ocopies[other].start()

        return carry

    lax.fori_loop(0, NX, last_body, 0)
    for j in (2, 3, 1):
        ocopies[j].wait_recv()

    tails = [osend[0, :, 128:].astype(F32)] + [orecv[j, :, 128:].astype(F32) for j in (1, 2, 3)]
    mains = [osend[0, :, :128]] + [orecv[j, :, :128] for j in (1, 2, 3)]

    def weigh(a):
        levels = [(t[:, a : a + 1] + t[:, a + 1 : a + 2]) + t[:, a + 2 : a + 3] for t in tails]
        best = functools.reduce(jnp.maximum, levels)
        portions = [jnp.exp2(level - best) for level in levels]
        total = functools.reduce(jnp.add, portions)
        return [portion / total for portion in portions]

    merged_w = functools.reduce(jnp.add, [m.astype(F32) * s for m, s in zip(mains, weigh(64))])
    merged_n = functools.reduce(jnp.add, [t * s for t, s in zip(tails, weigh(67))])
    ysend[:, :128] = merged_w.astype(BF)
    ysend[:, 128:] = jnp.where(lane_q < 64, merged_n, 0.0).astype(BF)
    hcopies = {}
    for j in (2, 1, 3):
        part = pl.ds(pl.multiple_of(lax.rem(y + j, NT) * SUB, SUB), SUB)
        hcopies[j] = send(ysend.at[part], yrecv.at[j], h_ss.at[j], h_rs.at[j], ys[j])

    own = ysend[pl.ds(pl.multiple_of(y * SUB, SUB), SUB)]
    proj = mm(own[:, :192], wbuf[0]).astype(BF).astype(F32)
    for j, needed in ((1, (0,)), (3, (1,)), (2, (2, 3))):
        if j == 2:
            for copy in needed:
                wcopies[copy].wait_recv()
        hcopies[j].wait_recv()
        proj = proj + mm(yrecv[j, :, :192], wbuf[j]).astype(BF).astype(F32)
    stream = (rbuf[...].astype(F32) + rms_scale(proj, attn_gain[...])).astype(BF)
    mixed_ref[...] = stream
    moe_in[...] = rms_scale(stream.astype(F32), ffn_gain[...]).astype(BF)

    z_order = (4, 3, 5, 2, 6, 1, 7)
    x_order = (4, 5, 2, 3, 6, 7, 1)

    def seg(number):
        return pl.ds(pl.multiple_of(number * 8, 8), 8)

    def across_lanes(c):
        return pl.ds(0, PIECES[c][2])

    def over_z(src, dst, c, local_sem, ss, rs):
        copies = {
            d: send(
                src.at[c, seg(zs[d]), across_lanes(c)],
                dst.at[c, seg(z), across_lanes(c)],
                ss.at[c, d],
                rs.at[c, d],
                {"sp_0": zs[d]},
            )
            for d in z_order
        }
        kept = pltpu.make_async_copy(
            src.at[c, seg(z), across_lanes(c)], dst.at[c, seg(z), across_lanes(c)], local_sem.at[c]
        )
        kept.start()
        return copies, kept

    def over_x(src, dst, c, local_sem, ss, rs):
        copies = {}
        for d in x_order:
            a, b = gs[d]
            copies[d] = send(
                src(c, seg(a * NC + b)),
                dst(c, seg(mine)),
                ss.at[c, d],
                rs.at[c, d],
                {"sp_1": a, "sp_2": b},
            )
        kept = pltpu.make_async_copy(src(c, seg(mine)), dst(c, seg(mine)), local_sem.at[c])
        kept.start()
        return copies, kept

    def arrived(moved):
        copies, kept = moved
        kept.wait()
        for copy in copies.values():
            copy.wait_recv()

    def lanes(c):
        return slice(PIECES[c][1], PIECES[c][1] + PIECES[c][2])

    def here(c):
        return slice(0, PIECES[c][2])

    z_moves, x_moves, near, far = {}, {}, {}, {}
    sums, joined, back_x, back_z = {}, {}, {}, {}
    high, low, whole = pl.ds(0, HALF), pl.ds(HALF, HALF), pl.ds(0, ROWS)
    begun = set()

    def hop(src, src_at, dst, dst_at, part, ss, rs, n, where):
        c = src_at[0]
        return send(
            src.at[(*src_at, part, across_lanes(c))],
            dst.at[(*dst_at, part, across_lanes(c))],
            ss.at[c, n],
            rs.at[c, n],
            where,
        )

    branch_ref[...] = jnp.zeros((SUB, D), F32)
    for c in range(CHUNKS):
        place = placing(PIECES[c][0]).astype(BF)
        sbuf[c, :, here(c)] = mm(place, moe_in[:, lanes(c)]).astype(BF)
        z_moves[c] = over_z(sbuf, zbuf, c, zl_sem, z_ss, z_rs)

    def stage_z(c):
        arrived(z_moves[c])
        xsend[c, :, here(c)] = mm(order, zbuf[c, :, here(c)]).astype(BF)
        x_moves[c] = over_x(
            lambda c, s: xsend.at[c, s, across_lanes(c)],
            lambda c, s: rows.at[c, 0, s, across_lanes(c)],
            c,
            xl_sem,
            x_ss,
            x_rs,
        )

    def stage_x(c):
        arrived(x_moves[c])
        near[c] = (
            hop(rows, (c, 0), rows, (c, 1), whole, y_ss, y_rs, 0, right),
            hop(rows, (c, 0), rows, (c, 3), whole, y_ss, y_rs, 1, left),
        )

    def stage_near(c):
        near[c][0].wait_recv()
        one = hop(rows, (c, 1), rows, (c, 2), high, y_ss, y_rs, 2, right)
        near[c][1].wait_recv()
        two = hop(rows, (c, 3), rows, (c, 2), low, y_ss, y_rs, 3, left)
        far[c] = (one, two)

    def stage_gate(c):
        for copy in far[c]:
            copy.wait_recv()
        if not begun:
            loads[2].wait()
            loads[3].wait()
        slot = PIECES[c][0]
        fresh = slot not in begun
        begun.add(slot)

        def tile(n, carry):
            to = pl.ds(pl.multiple_of(n * HID, 128), HID)
            held = rows[c, :, :, here(c)].reshape(NT * ROWS, PIECES[c][2])
            part = mm(held, w_in[lanes(c), to])
            if fresh:
                accum[:, to] = part
            else:
                accum[:, to] += part
            return carry

        lax.fori_loop(0, 2, tile, 0)

    def stage_act(s):
        def some(b, carry):
            part = pl.ds(pl.multiple_of(b * 64, 64), 64)
            hidden[part] = (jax.nn.silu(accum[part, :HID]) * accum[part, HID:]).astype(BF)
            return carry

        lax.fori_loop(0, NT * ROWS // 64, some, 0)
        if s == 0:
            loads[4].wait()

    def stage_down(c):
        def tile(n, carry):
            to = pl.ds(pl.multiple_of(n * 256, 256), 256)
            at_lane = pl.ds(pl.multiple_of(PIECES[c][1] + n * 256, 256), 256)
            part = mm(hidden[...], w_out[:, at_lane]).astype(BF)
            pbuf[c, :, :, to] = part.reshape(NT, ROWS, 256)
            return carry

        lax.fori_loop(0, PIECES[c][2] // 256, tile, 0)
        sums[c] = [
            hop(pbuf, (c, 2), relay, (c, 0), high, r_ss, r_rs, 0, right),
            hop(pbuf, (c, 2), relay, (c, 0), low, r_ss, r_rs, 1, left),
            hop(pbuf, (c, 3), ring, (c, 0), low, r_ss, r_rs, 2, right),
            hop(pbuf, (c, 1), ring, (c, 1), high, r_ss, r_rs, 3, left),
        ]

    def stage_join(c):
        at_lanes = here(c)
        sums[c][0].wait_recv()
        pbuf[c, 3, :HALF, at_lanes] = (
            pbuf[c, 3, :HALF, at_lanes].astype(F32) + relay[c, 0, :HALF, at_lanes].astype(F32)
        ).astype(BF)
        one = hop(pbuf, (c, 3), ring, (c, 0), high, r_ss, r_rs, 4, right)
        sums[c][1].wait_recv()
        pbuf[c, 1, HALF:, at_lanes] = (
            pbuf[c, 1, HALF:, at_lanes].astype(F32) + relay[c, 0, HALF:, at_lanes].astype(F32)
        ).astype(BF)
        two = hop(pbuf, (c, 1), ring, (c, 1), low, r_ss, r_rs, 5, left)
        joined[c] = (one, two)

    def stage_sum(c):
        for copy in sums[c][2:] + list(joined[c]):
            copy.wait_recv()
        ebuf[c, :, here(c)] = (
            pbuf[c, 0, :, here(c)].astype(F32)
            + ring[c, 0, :, here(c)].astype(F32)
            + ring[c, 1, :, here(c)].astype(F32)
        ).astype(BF)
        back_x[c] = over_x(
            lambda c, s: ebuf.at[c, s, across_lanes(c)],
            lambda c, s: xback.at[c, s, across_lanes(c)],
            c,
            bl_sem,
            bx_ss,
            bx_rs,
        )

    def stage_back(c):
        arrived(back_x[c])
        zsend[c, :, here(c)] = mm(order_back, xback[c, :, here(c)]).astype(BF)
        back_z[c] = over_z(zsend, zback, c, cl_sem, bz_ss, bz_rs)

    def stage_pick(c):
        arrived(back_z[c])
        s = PIECES[c][0]
        back = zback[c, :, here(c)]
        branch_ref[:, lanes(c)] += share[0] * mm(picking(0, s), back) + share[1] * mm(
            picking(1, s), back
        )

    stages = {
        "z": stage_z,
        "x": stage_x,
        "near": stage_near,
        "gate": stage_gate,
        "act": stage_act,
        "down": stage_down,
        "join": stage_join,
        "sum": stage_sum,
        "back": stage_back,
        "pick": stage_pick,
    }
    for line in STAGES:
        for word in line.split():
            stages[word[:-1]](int(word[-1]))

    mixed_ref[...] = (
        mixed_ref[...].astype(F32) + rms_scale(branch_ref[...], moe_gain[...])
    ).astype(BF)

    for moves in (z_moves, x_moves, back_x, back_z):
        for copies, _ in moves.values():
            for copy in copies.values():
                copy.wait_send()
    for group in (near, far, sums, joined):
        for copies in group.values():
            for copy in copies:
                copy.wait_send()
    for group in (fwd, bwd, across, qcopies, ocopies, hcopies):
        for copy in group.values():
            copy.wait_send()
    for copy in wcopies:
        copy.wait_send()


def layer(*args):
    dma = pltpu.SemaphoreType.DMA
    vmem = pl.BlockSpec(memory_space=pltpu.VMEM)
    hbm = pl.BlockSpec(memory_space=pl.ANY)
    buf = pltpu.VMEM((CHUNKS, ROWS, WIDE), BF)
    return pl.pallas_call(
        layer_kernel,
        out_shape=jax.ShapeDtypeStruct((SUB, D), BF),
        in_specs=[vmem] * 7 + [hbm] * 5 + [vmem] * 5 + [hbm] * 5,
        out_specs=vmem,
        scratch_shapes=[
            pltpu.VMEM((SUB, D), F32),
            pltpu.VMEM((2, 256, 128), BF),
            pltpu.VMEM((SUB, D), BF),
            pltpu.VMEM((NX, TOK, 384), BF),
            pltpu.VMEM((NZ, NC, TOK + ROPE, 256), BF),
            pltpu.VMEM((256, 512), BF),
            pltpu.VMEM((6 * TOK, 256), BF),
            pltpu.VMEM((6 * TOK, 128), BF),
            pltpu.VMEM((6 * TOK, 256), BF),
            pltpu.VMEM((6 * TOK, 128), BF),
            pltpu.VMEM((NX, TOK, 128), F32),
            pltpu.VMEM((NX, TOK, 128), F32),
            pltpu.VMEM((NX, TOK, 256), F32),
            pltpu.VMEM((NX, TOK, 128), F32),
            pltpu.VMEM((NX, TOK, 256), BF),
            pltpu.VMEM((NX, TOK, 256), BF),
            pltpu.VMEM((TOK, 256), BF),
            pltpu.VMEM((NT, SUB, 256), BF),
            pltpu.VMEM((NT, 192, D), BF),
            pltpu.VMEM((SUB, D), BF),
            buf,
            buf,
            buf,
            pltpu.VMEM((CHUNKS, NT, ROWS, WIDE), BF),
            pltpu.VMEM((D, 2 * HID), BF),
            pltpu.VMEM((HID, D), BF),
            pltpu.VMEM((NT * ROWS, 2 * HID), F32),
            pltpu.VMEM((NT * ROWS, HID), BF),
            pltpu.VMEM((CHUNKS, NT, ROWS, WIDE), BF),
            pltpu.VMEM((CHUNKS, 1, ROWS, WIDE), BF),
            pltpu.VMEM((CHUNKS, 2, ROWS, WIDE), BF),
            buf,
            buf,
            buf,
            buf,
            dma((10,)),
            dma((NX,)),
            dma((NX,)),
            dma((5, 2)),
            dma((5, 2)),
            dma((5, 2)),
            dma((5, 2)),
            dma((9,)),
            dma((9,)),
            dma((NX,)),
            dma((NX,)),
            dma((NT,)),
            dma((NT,)),
            dma((4,)),
            dma((4,)),
            dma((CHUNKS,)),
            dma((CHUNKS, NZ)),
            dma((CHUNKS, NZ)),
            dma((CHUNKS,)),
            dma((CHUNKS, GROUP)),
            dma((CHUNKS, GROUP)),
            dma((CHUNKS, 4)),
            dma((CHUNKS, 4)),
            dma((CHUNKS, 6)),
            dma((CHUNKS, 6)),
            dma((CHUNKS,)),
            dma((CHUNKS, GROUP)),
            dma((CHUNKS, GROUP)),
            dma((CHUNKS,)),
            dma((CHUNKS, NZ)),
            dma((CHUNKS, NZ)),
        ],
        compiler_params=pltpu.CompilerParams(
            collective_id=0, has_side_effects=True, vmem_limit_bytes=58 * 1024 * 1024
        ),
        name="layer",
    )(*args)


def local(
    resid,
    query_wide,
    query_narrow,
    latent,
    rope_key,
    latent_gain,
    key_up_wide,
    value_up_wide,
    key_up_narrow,
    value_up_narrow,
    out_wide,
    out_narrow,
    attn_gain,
    ffn_gain,
    moe_gain,
    routes,
    route_logit,
    expert_gate,
    expert_up,
    expert_down,
):
    positions = lax.axis_index(SP) * TOK + jnp.arange(TOK, dtype=jnp.int32)
    freq = THETA ** (-jnp.arange(ROPE // 2, dtype=jnp.float32) * 2.0 / ROPE)
    angle = freq[:, None] * positions.astype(jnp.float32)[None, :]
    return layer(
        latent,
        latent_gain[None],
        rope_key.T,
        query_wide.T,
        query_narrow,
        jnp.cos(angle),
        jnp.sin(angle),
        key_up_wide,
        value_up_wide,
        key_up_narrow,
        value_up_narrow,
        resid,
        attn_gain[None],
        ffn_gain[None],
        moe_gain[None],
        routes.T,
        route_logit.T,
        out_wide,
        out_narrow,
        expert_gate,
        expert_up,
        expert_down,
    )


def solution(mesh):
    split = Mesh(mesh.devices.reshape(8, 4, 2, mesh.shape["tp"]), ("sp_0", "sp_1", "sp_2", "tp"))
    in_specs = (
        P(SP_TP, None),
        P(SP, "tp"),
        P(SP, "tp"),
        P(SP, None),
        P(SP, None),
        P(),
        P(),
        P(),
        P(),
        P(),
        P("tp", None),
        P("tp", None),
        P(),
        P(),
        P(),
        P(SP_TP, None),
        P(SP_TP, None),
        P(SP, None, "tp"),
        P(SP, None, "tp"),
        P(SP, "tp", None),
    )
    out_specs = P(SP_TP, None)
    return jax.shard_map(local, mesh=split, in_specs=in_specs, out_specs=out_specs, check_vma=False)
```
